32 devices in a mesh: rep: 4 (over z), fs: 4 (over y, x), tp: 2 (over core).
Axes of the slice: x: 2, y: 2, z: 4, core: 2. Of those that a mesh axis runs over, the one named last changes fastest.
Arguments:
- tokens: bfloat16 [8192, 2048], P(('rep', 'fs')), may hold values from -6 to 6
- mix_gain: float32 [2048], replicated, may hold values from 0.1 to 1.9
- w_gate_b: bfloat16 [2048, 1024], P('fs', 'tp'), may hold values from -0.125 to 0.125
- w_gate_c: bfloat16 [2048, 1024], P('fs', 'tp'), may hold values from -0.125 to 0.125
- w_conv_in: bfloat16 [2048, 1024], P('fs', 'tp'), may hold values from -0.125 to 0.125
- conv_taps: float32 [3, 1024], P(None, 'tp'), may hold values from -3 to 3
- w_mix_out: bfloat16 [1024, 2048], P('tp', 'fs'), may hold values from -0.1875 to 0.1875
- ffn_gain: float32 [2048], replicated, may hold values from 0.1 to 1.9
- w_ffn_gate: bfloat16 [2048, 2816], P('fs', 'tp'), may hold values from -0.125 to 0.125
- w_ffn_up: bfloat16 [2048, 2816], P('fs', 'tp'), may hold values from -0.125 to 0.125
- w_ffn_down: bfloat16 [2816, 2048], P('tp', 'fs'), may hold values from -0.109375 to 0.109375
Outputs:
- layer_out: bfloat16 [8192, 2048], P(('rep', 'fs', 'tp'))
The draws below stay inside these ranges and needn't reach their ends.
All inputs are finite; a program needn't handle non-finite values.
Results may differ from the reference program's by a relative error of at most 0.014.
Values may be sent and summed in bfloat16 or wider, within the bound.
A program may use at most 64 MiB of HBM per device.

```python
import jax
import jax.numpy as jnp
from jax import lax

D = 2048
DC = 1024
FF = 2816
LEN = 128
TOKENS = 8192
N_TP = 2


def shard_levels(own_key, shape, pieces, smallest, top_value):
    loudness = 1.0
    for dim, parts in pieces:
        draws = jax.random.uniform(jax.random.fold_in(jax.random.fold_in(own_key, 6), dim), (parts,), jnp.float32, smallest / len(pieces), top_value / len(pieces))
        loudness = loudness * jnp.repeat(jnp.exp(draws), shape[dim] // parts).reshape((-1,) + (1,) * (len(shape) - 1 - dim))
    return loudness


def gaussian(rng, shape, scale, limit, cuts=(), held_as=jnp.bfloat16):
    loudness = shard_levels(rng, shape, cuts, -0.22, 0.18) if cuts else 1.0
    values = jax.random.normal(rng, shape, jnp.float32) * scale * loudness
    return jnp.minimum(jnp.maximum(values, -limit), limit).astype(held_as)


def setup_inputs(seed: int = 0) -> dict:
    keys = jax.random.split(jax.random.key(seed), 12)
    tokens = gaussian(keys[0], (TOKENS, D), 1.0, 6.0, ((0, 16),))
    mix_gain = jnp.clip(1.0 + 0.18 * jax.random.normal(keys[1], (D,), jnp.float32), 0.1, 1.9)
    w_gate_b = gaussian(keys[2], (D, DC), D ** -0.5, 0.125, ((0, 4), (1, 2)))
    w_gate_c = gaussian(keys[3], (D, DC), D ** -0.5, 0.125, ((0, 4), (1, 2)))
    w_conv_in = gaussian(keys[4], (D, DC), D ** -0.5, 0.125, ((0, 4), (1, 2)))
    conv_taps = gaussian(keys[5], (3, DC), 0.6, 3.0, ((1, 2),), jnp.float32)
    w_mix_out = gaussian(keys[6], (DC, D), DC ** -0.5, 0.1875, ((0, 2), (1, 4)))
    ffn_gain = jnp.clip(1.0 + 0.18 * jax.random.normal(keys[7], (D,), jnp.float32), 0.1, 1.9)
    w_ffn_gate = gaussian(keys[8], (D, FF), D ** -0.5, 0.125, ((0, 4), (1, 2)))
    w_ffn_up = gaussian(keys[9], (D, FF), D ** -0.5, 0.125, ((0, 4), (1, 2)))
    w_ffn_down = gaussian(keys[10], (FF, D), FF ** -0.5, 0.109375, ((0, 2), (1, 4)))
    return {"tokens": tokens, "mix_gain": mix_gain, "w_gate_b": w_gate_b, "w_gate_c": w_gate_c, "w_conv_in": w_conv_in, "conv_taps": conv_taps, "w_mix_out": w_mix_out, "ffn_gain": ffn_gain, "w_ffn_gate": w_ffn_gate, "w_ffn_up": w_ffn_up, "w_ffn_down": w_ffn_down}


EPSILON = 1e-06

def rms_scale(values, gain):
    return values * lax.rsqrt(lax.optimization_barrier(jnp.mean(values * values, axis=-1, keepdims=True)) + EPSILON) * gain

def causal_mix(product_in, conv_taps):
    shaped = product_in.reshape(product_in.shape[0] // LEN, LEN, product_in.shape[1])
    padded = jnp.pad(shaped, ((0, 0), (2, 0), (0, 0)))
    convolved = conv_taps[0] * padded[:, :-2] + conv_taps[1] * padded[:, 1:-1] + conv_taps[2] * padded[:, 2:]
    return convolved.reshape(product_in.shape)

def block_sum(acts, weight, blocks):
    block_width = acts.shape[1] // blocks

    def step(running, block_index):
        first = (block_index * block_width).astype(jnp.int32)
        partial_value = jnp.dot(lax.dynamic_slice_in_dim(acts, first, block_width, 1), lax.dynamic_slice_in_dim(weight, first, block_width, 0), preferred_element_type=jnp.float32)
        rounded = lax.optimization_barrier(partial_value.astype(jnp.bfloat16)).astype(jnp.float32)
        return (running + rounded, None)
    start_acc = jnp.zeros((acts.shape[0], weight.shape[1]), jnp.float32)
    running, _ = lax.scan(step, start_acc, jnp.arange(blocks, dtype=jnp.int32))
    return running

def reference(tokens, mix_gain, w_gate_b, w_gate_c, w_conv_in, conv_taps, w_mix_out, ffn_gain, w_ffn_gate, w_ffn_up, w_ffn_down):
    inputs = tokens.astype(jnp.float32)
    normed = rms_scale(inputs, mix_gain).astype(jnp.bfloat16)
    gate_b = jnp.dot(normed, w_gate_b, preferred_element_type=jnp.float32)
    gate_c = jnp.dot(normed, w_gate_c, preferred_element_type=jnp.float32)
    conv_in = jnp.dot(normed, w_conv_in, preferred_element_type=jnp.float32)
    convolved = causal_mix(gate_c * conv_in, conv_taps)
    gated = (gate_b * convolved).astype(jnp.bfloat16)
    stream = inputs + block_sum(gated, w_mix_out, N_TP)
    normed_two = rms_scale(stream, ffn_gain).astype(jnp.bfloat16)
    gate_part = jnp.dot(normed_two, w_ffn_gate, preferred_element_type=jnp.float32)
    up_part = jnp.dot(normed_two, w_ffn_up, preferred_element_type=jnp.float32)
    hidden = (jax.nn.silu(gate_part) * up_part).astype(jnp.bfloat16)
    return (stream + block_sum(hidden, w_ffn_down, N_TP)).astype(jnp.bfloat16)
```

```python
import jax
import jax.numpy as jnp
from jax import lax
from jax.experimental import pallas as pl
from jax.experimental.pallas import tpu as pltpu
from jax.sharding import PartitionSpec as P

LEN = 128
LANES = 128
EPSILON = 1e-06
MESH = pl.DeviceIdType.MESH
F32 = jnp.float32
BF16 = jnp.bfloat16


def rms_scale(values, gain):
    return values * lax.rsqrt(jnp.mean(values * values, axis=-1, keepdims=True) + EPSILON) * gain


N_CHUNKS = 4
TILE = 16


def inner_units(hidden):
    units = hidden // LANES
    return (7 * units + 5) // 11


def tiles(rows, share):
    return int(rows * share) // TILE * TILE


def weight_pieces(role, rows_d, n_conv, mix_rows, n_mix, units, hid, n_down):
    third = 1 / 3
    pieces = [(0, i * rows_d // 2, rows_d // 2, 0, n_conv, third) for i in range(2)]
    pieces += [(1, i * mix_rows // 2, mix_rows // 2, 0, n_mix, third) for i in range(2)]
    cuts = [i * units // 4 for i in range(4)] + [units]
    if role:
        cuts = [(2 * i * units + 6) // 7 for i in range(4)] + [units]
    pieces += [(2, 0, rows_d, 2 * LANES * a, 2 * LANES * (b - a), third) for a, b in zip(cuts, cuts[1:])]
    down = (0, n_down // 2, 3 * n_down // 4, n_down)
    for a, b, share in zip(down, down[1:], (third, 0.29, 0.22)):
        pieces.append((3, 0, hid, a, b - a, share))
    return pieces


N_PIECES = 11


def layer_kernel(*refs):
    r = lax.axis_index("rep")
    p = lax.rem(r, 2)
    f = lax.axis_index("fs")
    barrier = pltpu.get_barrier_semaphore()
    x_of = f + 1 - 2 * lax.rem(f, 2)
    for dev in (
        {"fs": x_of}, {"fs": lax.rem(f + 2, 4)}, {"rep": r + 1 - 2 * p}, {"tp": 1 - lax.axis_index("tp")}
    ):
        pl.semaphore_signal(barrier, inc=1, device_id=dev, device_id_type=MESH)
    inner = jnp.logical_or(r == 1, r == 2)

    @pl.when(inner)
    def _():
        layer_body(1, barrier, *refs)

    @pl.when(jnp.logical_not(inner))
    def _():
        layer_body(0, barrier, *refs)


def layer_body(
    role, barrier,
    tokens, wb, wc, wi, wm_in, wg_in, wu_in, wd_in, mix_gain_in, taps_in, ffn_gain_in,
    out,
    tok, normed, n2, WA, WM, WG, WD, gated, MP, RS, BR, hidden, OP, RO, ZC, RF, mix_gain, taps, ffn_gain,
    load_sem, ds, dr, fs_, fr, us, ur, tz_s, tz_r, ts_s, ts_r, g_s, g_r, sib_s, sib_r, z_s, z_r, n_s, n_r,
    o_s, o_r, q_s, q_r,
):
    n_fs, rows_d, _ = WA.shape
    ch = gated.shape[2]
    width = tokens.shape[1]
    half = tokens.shape[0] // 4
    cols = WD.shape[2]
    mcols = WM.shape[2]
    all_units = wg_in.shape[1] // LANES
    units = inner_units(wg_in.shape[1])
    first = 0
    if not role:
        first, units = units, all_units - units
    hid = units * LANES

    r = lax.axis_index("rep")
    f = lax.axis_index("fs")
    t = lax.axis_index("tp")
    p = lax.rem(r, 2)
    twin = r - 1
    z_dev = {"rep": r + 1 - 2 * p}
    w_dev = {"rep": 3 - r}
    x_of = f + 1 - 2 * lax.rem(f, 2)
    y_of = lax.rem(f + 2, 4)
    d_of = lax.rem(x_of + 2, 4)
    x_dev, y_dev, s_dev = {"fs": x_of}, {"fs": y_of}, {"tp": 1 - t}

    def part(c, core):
        return pl.ds(pl.multiple_of((2 * c + core) * half, half), half)

    def chunk(c):
        return pl.ds(pl.multiple_of(2 * c * half, 2 * half), 2 * half)

    if role:
        pl.semaphore_signal(barrier, inc=1, device_id=w_dev, device_id_type=MESH)

    chan = pl.ds(role * ch, ch)
    loads = []

    def load(src, dst):
        c = pltpu.make_async_copy(src, dst, load_sem.at[len(loads)])
        c.start()
        loads.append(c)
        return c

    l_wa = []
    for k in range(2):
        rows = pl.ds(k * (rows_d // 2), rows_d // 2)
        l_wa.append([
            load(w.at[rows, chan], WA.at[f, rows, pl.ds(i * ch, ch)]) for i, w in enumerate((wb, wc, wi))
        ])
    l_tok = [
        load(tokens.at[pl.ds((2 * core + h) * half, half)], tok.at[part(2 * h + p, core)])
        for h in range(2) for core in range(2)
    ]
    l_small = [
        load(a, b) for a, b in ((mix_gain_in, mix_gain), (taps_in, taps), (ffn_gain_in, ffn_gain))
    ]
    pl.semaphore_wait(barrier, 4 + role)

    def remote(src, dst, s, rcv, dev):
        return pltpu.make_async_remote_copy(
            src_ref=src, dst_ref=dst, send_sem=s, recv_sem=rcv, device_id=dev, device_id_type=MESH
        )

    bufs = (WA, WM, WG, WD)
    pieces = weight_pieces(role, rows_d, 3 * ch, WM.shape[1], mcols, units, hid, cols)

    def cut(k, slot, lo, n):
        w, r0, _, c0, nc, _ = pieces[k]
        at = r0 + lo
        if not isinstance(at, int):
            at = pl.multiple_of(at, TILE)
        return bufs[w].at[slot, pl.ds(at, n), pl.ds(c0, nc)]

    def share(k):
        rows = pieces[k][2]
        lent = tiles(rows, pieces[k][5]) if role else 0
        kept = rows - lent
        near = tiles(kept, 0.5)
        lo = twin * lent if role else 0
        mine = twin * kept if role else 0
        return lent, kept, near, lo, mine

    def direct(k):
        _, kept, _, lo, _ = share(k)
        ref = cut(k, f, lo, kept)
        return [remote(ref, ref, ds.at[k, c], dr.at[k, c], dev) for c, dev in ((0, x_dev), (1, y_dev))]

    def forward(k):
        _, kept, near, lo, _ = share(k)
        a, b = cut(k, x_of, lo, near), cut(k, y_of, lo + near, kept - near)
        return [
            remote(b, b, fs_.at[k, 0], fr.at[k, 0], x_dev),
            remote(a, a, fs_.at[k, 1], fr.at[k, 1], y_dev),
        ]

    def lend(k, *slots):
        lent, _, _, _, mine = share(k)
        refs = {0: x_of, 1: y_of, 2: d_of}
        copies = []
        for s in slots:
            ref = cut(k, refs[s], mine, lent)
            copies.append(remote(ref, ref, us.at[k, s], ur.at[k, s], w_dev))
        return copies

    sent = []

    def start(*copies):
        for c in copies:
            c.start()
            sent.append(c)
        return copies

    D, F, Z, ZD = {}, {}, {}, {}

    def send(*ks):
        for k in ks:
            D[k] = start(*direct(k))

    def step(k, *more):
        for c in D[k]:
            c.wait_recv()
        F[k] = start(*forward(k))
        if role:
            Z[k] = start(*lend(k, 0, 1))
        send(*more)

    def across(*ks):
        for k in ks:
            if k not in ZD:
                for c in F[k]:
                    c.wait_recv()
                ZD[k] = start(*lend(k, 2)) if role else ()

    def sides(*ks):
        if role:
            for k in ks:
                for c in Z[k]:
                    c.wait_recv()

    def corner(*ks):
        across(*ks)
        for k in ks:
            for c in ZD[k]:
                c.wait_recv()

    def arrived(*ks):
        across(*ks)
        sides(*ks)
        corner(*ks)

    for k in range(2):
        for c in l_wa[k]:
            c.wait()
        send(k)
    for c in l_tok + l_small:
        c.wait()
    tz, ts = [], []
    for h in range(2):
        ref = tok.at[part(2 * h + p, t)]
        tz += start(remote(ref, ref, tz_s.at[h], tz_r.at[h], z_dev))

    def relay(h):
        tz[h].wait_recv()
        ref = tok.at[part(2 * h + 1 - p, t)]
        ts.extend(start(remote(ref, ref, ts_s.at[h], ts_r.at[h], s_dev)))

    def norm_chunk(c):
        def body(i, _):
            rows = pl.ds(pl.multiple_of(2 * c * half + i * 64, 64), 64)
            normed[rows, :] = rms_scale(tok[rows, :].astype(F32), mix_gain[...]).astype(BF16)
            return 0

        lax.fori_loop(0, 2 * half // 64, body, 0)

    l_rest = [load(wm_in.at[:, pl.ds(role * mcols, mcols)], WM.at[f])]
    for c in range(units):
        for i, w in enumerate((wg_in, wu_in)):
            l_rest.append(load(
                w.at[:, pl.ds((first + c) * LANES, LANES)], WG.at[f, :, pl.ds((2 * c + i) * LANES, LANES)]
            ))
    l_rest.append(load(wd_in.at[pl.ds(first * LANES, hid)], WD.at[f, pl.ds(0, hid)]))

    norm_chunk(p)
    norm_chunk(2 + p)
    for c in l_rest:
        c.wait()
    step(0)
    relay(0)
    step(1, 2, 3, *((4,) if role else ()))
    ts[0].wait_recv()
    norm_chunk(1 - p)
    across(0)
    relay(1)
    ts[1].wait_recv()
    norm_chunk(3 - p)
    arrived(0, 1)

    tap = [taps[pl.ds(i, 1), chan] for i in range(3)]
    pos = lax.rem(lax.broadcasted_iota(jnp.int32, (2 * half, ch), 0), LEN)

    def mix_in(c):
        x = normed[chunk(c), :]

        def proj(q):
            w = WA[:, :, q * ch:(q + 1) * ch].reshape(width, ch)
            return jnp.dot(x, w, preferred_element_type=F32)

        pr = proj(1) * proj(2)
        one = jnp.where(pos >= 1, pltpu.roll(pr, 1, 0), 0.0)
        two = jnp.where(pos >= 2, pltpu.roll(pr, 2, 0), 0.0)
        conv = tap[0] * two + tap[1] * one + tap[2] * pr
        gated[role, chunk(c), :] = (proj(0) * conv).astype(BF16)
        ref = gated.at[role, chunk(c)]
        gz.extend(start(remote(ref, ref, g_s.at[c], g_r.at[c], z_dev)))

    gz, sib, zc, nb = [], [], [], []

    def mix_out(c):
        gz[c].wait_recv()
        g = jnp.concatenate([gated[0, chunk(c), :], gated[1, chunk(c), :]], axis=1)
        for s in range(n_fs):
            MP[chunk(c), s * mcols:(s + 1) * mcols] = jnp.dot(
                g, WM[s], preferred_element_type=F32
            ).astype(BF16)
        sib.extend(start(remote(MP.at[part(c, 1 - t)], RS.at[c], sib_s.at[c], sib_r.at[c], s_dev)))

    def mix_pair(c):
        sib[c].wait_recv()
        BR[role, c] = (MP[part(c, t), :].astype(F32) + RS[c].astype(F32)).astype(BF16)
        zc.extend(start(remote(BR.at[role, c], BR.at[role, c], z_s.at[c], z_r.at[c], z_dev)))

    def stream_chunk(c):
        zc[c].wait_recv()
        step_rows = 32

        def body(i, _):
            rows = pl.ds(pl.multiple_of(i * step_rows, step_rows), step_rows)
            mine = pl.ds(pl.multiple_of((2 * c + t) * half + i * step_rows, step_rows), step_rows)
            branch = jnp.concatenate(
                [BR[q, c, rows, s * mcols:(s + 1) * mcols] for s in range(n_fs) for q in range(2)], axis=1
            )
            stream = tok[mine, :].astype(F32) + branch.astype(F32)
            n2[mine, :] = rms_scale(stream, ffn_gain[...]).astype(BF16)
            return 0

        lax.fori_loop(0, half // step_rows, body, 0)
        ref = n2.at[part(c, t)]
        nb.extend(start(remote(ref, ref, n_s.at[c], n_r.at[c], s_dev)))

    def ffn_rows(k, i):
        _, _, _, c0, nc, _ = pieces[k]
        rows = pl.ds(4 * i * half, 4 * half)
        x = n2[rows, :]
        for a in range(c0, c0 + nc, 2 * LANES):
            w = WG[:, :, a:a + 2 * LANES].reshape(width, 2 * LANES)
            zz = jnp.dot(x, w, preferred_element_type=F32)
            g, u = zz[:, :LANES], zz[:, LANES:]
            hidden[rows, a // 2:a // 2 + LANES] = (g / (1.0 + jnp.exp(-g)) * u).astype(BF16)

    mix_in(0)
    mix_in(1)
    step(2)
    mix_in(2)
    mix_in(3)
    step(3, *((5,) if role else (4, 5)))
    across(1)
    arrived(2, 3)
    mix_out(0)
    mix_out(1)
    mix_pair(0)
    mix_out(2)
    mix_pair(1)
    step(4, 6)
    mix_out(3)
    mix_pair(2)
    mix_pair(3)
    stream_chunk(0)
    step(5, 7)
    across(4)
    stream_chunk(1)
    for c in nb[:2]:
        c.wait_recv()
    arrived(4)
    ffn_rows(4, 0)
    step(6, 8)
    across(5)
    stream_chunk(2)
    arrived(5)
    ffn_rows(5, 0)
    stream_chunk(3)
    step(7, 9)
    across(6)
    for c in nb[2:]:
        c.wait_recv()
    ffn_rows(4, 1)
    ffn_rows(5, 1)
    arrived(6)
    ffn_rows(6, 0)
    ffn_rows(6, 1)
    step(8, 10)
    arrived(7)
    ffn_rows(7, 0)
    ffn_rows(7, 1)

    cuts = [pieces[k][3:5] for k in (8, 9, 10)]
    blocks = [(f, 0, cols)]
    blocks += [(x_of, *cuts[0]), (y_of, *cuts[0])]
    blocks += [(x_of, *cuts[1]), (y_of, *cuts[1]), (d_of, *cuts[0])]
    blocks += [(x_of, *cuts[2]), (y_of, *cuts[2]), (d_of, *cuts[1]), (d_of, *cuts[2])]
    so, qo = [], []

    def down_send(*ks):
        for k in ks:
            s, c0, nc = blocks[k]
            cs = pl.ds(c0, nc)

            def body(i, _, s=s, c0=c0, nc=nc):
                rows = pl.ds(pl.multiple_of(4 * i * half, 4 * half), 4 * half)
                prod = jnp.dot(
                    hidden[rows, :hid], WD[s, :hid, c0:c0 + nc], preferred_element_type=F32
                ).astype(BF16)
                for e in range(4):
                    OP[s, e % 2, 2 * i + e // 2, :, c0:c0 + nc] = prod[e * half:(e + 1) * half]
                return 0

            lax.fori_loop(0, N_CHUNKS // 2, body, 0)
            so.extend(start(remote(
                OP.at[s, 1 - t, :, :, cs], RO.at[s, :, :, cs], o_s.at[k], o_r.at[k], s_dev
            )))

    def down_pair(*ks):
        for k in ks:
            so[k].wait_recv()
            s, c0, nc = blocks[k]
            cs = pl.ds(c0, nc)
            for h in range(2):
                c = 2 * h + 1 - p
                ZC[s, h, :, cs] = (OP[s, t, c, :, cs].astype(F32) + RO[s, c, :, cs].astype(F32)).astype(BF16)
            qo.extend(start(remote(
                ZC.at[s, :, :, cs], RF.at[s, :, :, cs], q_s.at[k], q_r.at[k], z_dev
            )))

    def finish(*ks):
        for k in ks:
            qo[k].wait_recv()
            s, c0, nc = blocks[k]
            for a in range(0, nc, LANES):
                lo = c0 + a
                q, at = lo // mcols, lo % mcols
                cs = pl.ds(lo, LANES)
                ms = pl.ds(pl.multiple_of(s * mcols + at, LANES), LANES)
                whole = pl.ds(pl.multiple_of(s * cols + lo, LANES), LANES)
                for h in range(2):
                    c = 2 * h + p
                    stream = tok[part(c, t), whole].astype(F32) + BR[q, c, :, ms].astype(F32)
                    branch = (
                        OP[s, t, c, :, cs].astype(F32)
                        + RO[s, c, :, cs].astype(F32)
                        + RF[s, h, :, cs].astype(F32)
                    )
                    out[h * half:(h + 1) * half, whole] = (stream + branch).astype(BF16)

    down_send(0)
    across(7)
    step(9)
    down_pair(0)
    sides(8)
    down_send(1, 2)
    down_pair(1, 2)
    across(8)
    step(10)
    sides(9)
    down_send(3, 4)
    down_pair(3, 4)
    across(9)
    corner(8)
    down_send(5)
    down_pair(5)
    across(10)
    sides(10)
    down_send(6, 7)
    down_pair(6, 7)
    finish(0, 1, 2)
    corner(9)
    down_send(8)
    down_pair(8)
    finish(3, 4)
    corner(10)
    down_send(9)
    down_pair(9)
    finish(5, 6, 7, 8, 9)
    for c in sent:
        c.wait_send()


def paired_local(
    tokens, mix_gain, w_gate_b, w_gate_c, w_conv_in, conv_taps, w_mix_out, ffn_gain,
    w_ffn_gate, w_ffn_up, w_ffn_down,
):
    chip_rows, width = tokens.shape
    n_fs = lax.axis_size("fs")
    rows_d = w_gate_b.shape[0]
    ch = w_gate_b.shape[1] // 2
    units = inner_units(w_ffn_gate.shape[1])
    hid = units * LANES
    cols = w_mix_out.shape[1]
    half = chip_rows // 4
    group = 2 * chip_rows
    n_blocks = 10
    n_loads = 15 + 2 * units

    def vmem(*shape):
        return pltpu.VMEM(shape, BF16)

    def dma(*shape):
        return pltpu.SemaphoreType.DMA(shape)

    return pl.pallas_call(
        layer_kernel,
        out_shape=jax.ShapeDtypeStruct((2 * half, width), BF16),
        in_specs=[pl.BlockSpec(memory_space=pl.ANY)] * 11,
        out_specs=pl.BlockSpec(memory_space=pltpu.VMEM),
        scratch_shapes=[
            vmem(group, width),
            vmem(group, width),
            vmem(group, width),
            vmem(n_fs, rows_d, 3 * ch),
            vmem(n_fs, 2 * ch, cols // 2),
            vmem(n_fs, rows_d, 2 * hid),
            vmem(n_fs, hid, cols),
            vmem(2, group, ch),
            vmem(group, width // 2),
            vmem(N_CHUNKS, half, width // 2),
            vmem(2, N_CHUNKS, half, width // 2),
            vmem(group, hid),
            vmem(n_fs, 2, N_CHUNKS, half, cols),
            vmem(n_fs, N_CHUNKS, half, cols),
            vmem(n_fs, 2, half, cols),
            vmem(n_fs, 2, half, cols),
            pltpu.VMEM((1, width), F32),
            pltpu.VMEM(conv_taps.shape, F32),
            pltpu.VMEM((1, width), F32),
            dma(n_loads),
            *[dma(N_PIECES, 2)] * 4,
            *[dma(N_PIECES, 3)] * 2,
            *[dma(2)] * 4,
            *[dma(N_CHUNKS)] * 8,
            *[dma(n_blocks)] * 4,
        ],
        compiler_params=pltpu.CompilerParams(
            collective_id=0, has_side_effects=True, vmem_limit_bytes=60 * 2**20
        ),
    )(
        tokens, w_gate_b, w_gate_c, w_conv_in, w_mix_out, w_ffn_gate, w_ffn_up, w_ffn_down,
        mix_gain.reshape(1, width), conv_taps, ffn_gain.reshape(1, width),
    )


def causal_mix(product_in, conv_taps):
    shaped = product_in.reshape(product_in.shape[0] // LEN, LEN, product_in.shape[1])
    padded = jnp.pad(shaped, ((0, 0), (2, 0), (0, 0)))
    convolved = (
        conv_taps[0] * padded[:, :-2]
        + conv_taps[1] * padded[:, 1:-1]
        + conv_taps[2] * padded[:, 2:]
    )
    return convolved.reshape(product_in.shape)


def general_local(
    tokens, mix_gain, w_gate_b, w_gate_c, w_conv_in, conv_taps, w_mix_out, ffn_gain,
    w_ffn_gate, w_ffn_up, w_ffn_down,
):
    def scatter(product):
        return lax.psum_scatter(
            product.astype(BF16), "tp", scatter_dimension=0, tiled=True
        ).astype(F32)

    def dot(a, b):
        return jnp.dot(a, b, preferred_element_type=F32)

    def rows(w):
        return lax.all_gather(w, "fs", axis=0, tiled=True)

    normed = rms_scale(tokens.astype(F32), mix_gain).astype(BF16)
    gate_b, gate_c, conv_in = (dot(normed, rows(w)) for w in (w_gate_b, w_gate_c, w_conv_in))
    gated = (gate_b * causal_mix(gate_c * conv_in, conv_taps)).astype(BF16)
    row_count = normed.shape[0] // lax.axis_size("tp")
    branch = scatter(dot(gated, lax.all_gather(w_mix_out, "fs", axis=1, tiled=True)))
    own = lax.dynamic_slice_in_dim(tokens, lax.axis_index("tp") * row_count, row_count, 0)
    stream = own.astype(F32) + branch
    normed_two = lax.all_gather(
        rms_scale(stream, ffn_gain).astype(BF16), "tp", axis=0, tiled=True
    )
    hidden = (jax.nn.silu(dot(normed_two, rows(w_ffn_gate))) * dot(normed_two, rows(w_ffn_up))).astype(BF16)
    ffn_branch = scatter(dot(hidden, lax.all_gather(w_ffn_down, "fs", axis=1, tiled=True)))
    return (stream + ffn_branch).astype(BF16)


def solution(mesh):
    in_specs = (
        P(("rep", "fs"), None),
        P(),
        P("fs", "tp"),
        P("fs", "tp"),
        P("fs", "tp"),
        P(None, "tp"),
        P("tp", "fs"),
        P(),
        P("fs", "tp"),
        P("fs", "tp"),
        P("tp", "fs"),
    )
    out_specs = P(("rep", "fs", "tp"), None)
    size = mesh.shape
    square = size["tp"] == 2 and size["fs"] == 4 and size["rep"] == 4

    def local(*arrays):
        rows, width = arrays[0].shape
        channels, hidden = arrays[2].shape[1], arrays[8].shape[1]
        fits = (
            square
            and rows % (4 * LEN) == 0
            and channels % (2 * LANES) == 0
            and hidden % LANES == 0
            and hidden >= 11 * LANES
            and width % (16 * LANES) == 0
        )
        return (paired_local if fits else general_local)(*arrays)

    return jax.shard_map(local, mesh=mesh, in_specs=in_specs, out_specs=out_specs, check_vma=False)
```

```python
import jax
import jax.numpy as jnp
from jax import lax
from jax.experimental import pallas as pl
from jax.experimental.pallas import tpu as pltpu
from jax.sharding import PartitionSpec as P

LEN = 128
LANES = 128
EPSILON = 1e-06
MESH = pl.DeviceIdType.MESH
F32 = jnp.float32
BF16 = jnp.bfloat16


def rms_scale(values, gain):
    return values * lax.rsqrt(jnp.mean(values * values, axis=-1, keepdims=True) + EPSILON) * gain


N_CHUNKS = 4
TILE = 16


def inner_units(hidden):
    units = hidden // LANES
    return (7 * units + 5) // 11


def tiles(rows, share):
    return int(rows * share) // TILE * TILE


def weight_pieces(role, rows_d, n_conv, mix_rows, n_mix, units, hid, n_down):
    third = 1 / 3
    pieces = [(0, i * rows_d // 2, rows_d // 2, 0, n_conv, third) for i in range(2)]
    pieces += [(1, i * mix_rows // 2, mix_rows // 2, 0, n_mix, third) for i in range(2)]
    cuts = [i * units // 4 for i in range(4)] + [units]
    if role:
        cuts = [(u * units + 6) // 7 for u in (0, 1, 3, 5, 6)] + [units]
    pieces += [(2, 0, rows_d, 2 * LANES * a, 2 * LANES * (b - a), 0.32) for a, b in zip(cuts, cuts[1:])]
    down = (0, n_down // 2, 3 * n_down // 4, n_down)
    for a, b, share in zip(down, down[1:], (0.28, 0.25, 0.2)):
        pieces.append((3, 0, hid, a, b - a, share))
    return pieces


N_PIECES = 12


def layer_kernel(*refs):
    r = lax.axis_index("rep")
    p = lax.rem(r, 2)
    f = lax.axis_index("fs")
    barrier = pltpu.get_barrier_semaphore()
    x_of = f + 1 - 2 * lax.rem(f, 2)
    for dev in (
        {"fs": x_of}, {"fs": lax.rem(f + 2, 4)}, {"rep": r + 1 - 2 * p}, {"tp": 1 - lax.axis_index("tp")}
    ):
        pl.semaphore_signal(barrier, inc=1, device_id=dev, device_id_type=MESH)
    inner = jnp.logical_or(r == 1, r == 2)

    @pl.when(inner)
    def _():
        layer_body(1, barrier, *refs)

    @pl.when(jnp.logical_not(inner))
    def _():
        layer_body(0, barrier, *refs)


def layer_body(
    role, barrier,
    tokens, wb, wc, wi, wm_in, wg_in, wu_in, wd_in, mix_gain_in, taps_in, ffn_gain_in,
    out_hbm,
    out, tok, normed, n2, WA, WM, WG, WD, gated, MP, RS, BR, hidden, OP, RO, ZC, RF, mix_gain, taps, ffn_gain,
    load_sem, ds, dr, fs_, fr, us, ur, tz_s, tz_r, ts_s, ts_r, g_s, g_r, sib_s, sib_r, z_s, z_r, n_s, n_r,
    o_s, o_r, q_s, q_r, w_s,
):
    n_fs, rows_d, _ = WA.shape
    ch = gated.shape[2]
    width = tokens.shape[1]
    half = tokens.shape[0] // 4
    cols = WD.shape[2]
    mcols = WM.shape[2]
    all_units = wg_in.shape[1] // LANES
    units = inner_units(wg_in.shape[1])
    first = 0
    if not role:
        first, units = units, all_units - units
    hid = units * LANES

    r = lax.axis_index("rep")
    f = lax.axis_index("fs")
    t = lax.axis_index("tp")
    p = lax.rem(r, 2)
    twin = r - 1
    z_dev = {"rep": r + 1 - 2 * p}
    w_dev = {"rep": 3 - r}
    x_of = f + 1 - 2 * lax.rem(f, 2)
    y_of = lax.rem(f + 2, 4)
    d_of = lax.rem(x_of + 2, 4)
    x_dev, y_dev, s_dev = {"fs": x_of}, {"fs": y_of}, {"tp": 1 - t}

    def part(c, core):
        return pl.ds(pl.multiple_of((2 * c + core) * half, half), half)

    def chunk(c):
        return pl.ds(pl.multiple_of(2 * c * half, 2 * half), 2 * half)

    if role:
        pl.semaphore_signal(barrier, inc=1, device_id=w_dev, device_id_type=MESH)

    chan = pl.ds(role * ch, ch)
    loads = []

    def load(src, dst):
        c = pltpu.make_async_copy(src, dst, load_sem.at[len(loads)])
        c.start()
        loads.append(c)
        return c

    l_wa = []
    for k in range(2):
        rows = pl.ds(k * (rows_d // 2), rows_d // 2)
        l_wa.append([
            load(w.at[rows, chan], WA.at[f, rows, pl.ds(i * ch, ch)]) for i, w in enumerate((wb, wc, wi))
        ])
    l_tok = [
        load(tokens.at[pl.ds((2 * core + h) * half, half)], tok.at[part(2 * h + p, core)])
        for h in range(2) for core in range(2)
    ]
    l_small = [
        load(a, b) for a, b in ((mix_gain_in, mix_gain), (taps_in, taps), (ffn_gain_in, ffn_gain))
    ]
    pl.semaphore_wait(barrier, 4 + role)

    def remote(src, dst, s, rcv, dev):
        return pltpu.make_async_remote_copy(
            src_ref=src, dst_ref=dst, send_sem=s, recv_sem=rcv, device_id=dev, device_id_type=MESH
        )

    bufs = (WA, WM, WG, WD)
    pieces = weight_pieces(role, rows_d, 3 * ch, WM.shape[1], mcols, units, hid, cols)

    def cut(k, slot, lo, n):
        w, r0, _, c0, nc, _ = pieces[k]
        at = r0 + lo
        if not isinstance(at, int):
            at = pl.multiple_of(at, TILE)
        return bufs[w].at[slot, pl.ds(at, n), pl.ds(c0, nc)]

    def share(k):
        rows = pieces[k][2]
        lent = tiles(rows, pieces[k][5]) if role else 0
        kept = rows - lent
        near = tiles(kept, 0.5)
        lo = twin * lent if role else 0
        mine = twin * kept if role else 0
        return lent, kept, near, lo, mine

    def direct(k):
        _, kept, _, lo, _ = share(k)
        ref = cut(k, f, lo, kept)
        return [remote(ref, ref, ds.at[k, c], dr.at[k, c], dev) for c, dev in ((0, x_dev), (1, y_dev))]

    def forward(k):
        _, kept, near, lo, _ = share(k)
        a, b = cut(k, x_of, lo, near), cut(k, y_of, lo + near, kept - near)
        return [
            remote(b, b, fs_.at[k, 0], fr.at[k, 0], x_dev),
            remote(a, a, fs_.at[k, 1], fr.at[k, 1], y_dev),
        ]

    def lend(k, *slots):
        lent, _, _, _, mine = share(k)
        refs = {0: x_of, 1: y_of, 2: d_of}
        copies = []
        for s in slots:
            ref = cut(k, refs[s], mine, lent)
            copies.append(remote(ref, ref, us.at[k, s], ur.at[k, s], w_dev))
        return copies

    sent = []

    def start(*copies):
        for c in copies:
            c.start()
            sent.append(c)
        return copies

    D, F, Z, ZD = {}, {}, {}, {}

    def send(*ks):
        for k in ks:
            D[k] = start(*direct(k))

    def step(k, *more):
        for c in D[k]:
            c.wait_recv()
        F[k] = start(*forward(k))
        if role:
            Z[k] = start(*lend(k, 0, 1))
        send(*more)

    def across(*ks):
        for k in ks:
            if k not in ZD:
                for c in F[k]:
                    c.wait_recv()
                ZD[k] = start(*lend(k, 2)) if role else ()

    def sides(*ks):
        if role:
            for k in ks:
                for c in Z[k]:
                    c.wait_recv()

    def corner(*ks):
        across(*ks)
        for k in ks:
            for c in ZD[k]:
                c.wait_recv()

    def arrived(*ks):
        across(*ks)
        sides(*ks)
        corner(*ks)

    for k in range(2):
        for c in l_wa[k]:
            c.wait()
        send(k)
    for c in l_tok + l_small:
        c.wait()
    tz, ts = [], []
    for h in range(2):
        ref = tok.at[part(2 * h + p, t)]
        tz += start(remote(ref, ref, tz_s.at[h], tz_r.at[h], z_dev))

    def relay(h):
        tz[h].wait_recv()
        ref = tok.at[part(2 * h + 1 - p, t)]
        ts.extend(start(remote(ref, ref, ts_s.at[h], ts_r.at[h], s_dev)))

    def norm_chunk(c):
        def body(i, _):
            rows = pl.ds(pl.multiple_of(2 * c * half + i * 64, 64), 64)
            normed[rows, :] = rms_scale(tok[rows, :].astype(F32), mix_gain[...]).astype(BF16)
            return 0

        lax.fori_loop(0, 2 * half // 64, body, 0)

    l_rest = [load(wm_in.at[:, pl.ds(role * mcols, mcols)], WM.at[f])]
    for c in range(units):
        for i, w in enumerate((wg_in, wu_in)):
            l_rest.append(load(
                w.at[:, pl.ds((first + c) * LANES, LANES)], WG.at[f, :, pl.ds((2 * c + i) * LANES, LANES)]
            ))
    l_rest.append(load(wd_in.at[pl.ds(first * LANES, hid)], WD.at[f, pl.ds(0, hid)]))

    norm_chunk(p)
    norm_chunk(2 + p)
    for c in l_rest:
        c.wait()
    step(0)
    relay(0)
    if role:
        step(1, 2, 3)
        ts[0].wait_recv()
        norm_chunk(1 - p)
        across(0)
        across(1)
        step(2)
        step(3, 4, 5)
        relay(1)
        ts[1].wait_recv()
        norm_chunk(3 - p)
        across(2)
        across(3)
    else:
        ts[0].wait_recv()
        norm_chunk(1 - p)
        step(1, 2, 3)
        relay(1)
        ts[1].wait_recv()
        norm_chunk(3 - p)
    arrived(0, 1)

    tap = [taps[pl.ds(i, 1), chan] for i in range(3)]
    pos = lax.rem(lax.broadcasted_iota(jnp.int32, (2 * half, ch), 0), LEN)

    def mix_in(c):
        x = normed[chunk(c), :]

        def proj(q):
            w = WA[:, :, q * ch:(q + 1) * ch].reshape(width, ch)
            return jnp.dot(x, w, preferred_element_type=F32)

        pr = proj(1) * proj(2)
        one = jnp.where(pos >= 1, pltpu.roll(pr, 1, 0), 0.0)
        two = jnp.where(pos >= 2, pltpu.roll(pr, 2, 0), 0.0)
        conv = tap[0] * two + tap[1] * one + tap[2] * pr
        gated[role, chunk(c), :] = (proj(0) * conv).astype(BF16)
        ref = gated.at[role, chunk(c)]
        gz.extend(start(remote(ref, ref, g_s.at[c], g_r.at[c], z_dev)))

    gz, sib, zc, nb = [], [], [], []

    def mix_out(c):
        gz[c].wait_recv()
        g = jnp.concatenate([gated[0, chunk(c), :], gated[1, chunk(c), :]], axis=1)
        for s in range(n_fs):
            MP[chunk(c), s * mcols:(s + 1) * mcols] = jnp.dot(
                g, WM[s], preferred_element_type=F32
            ).astype(BF16)
        sib.extend(start(remote(MP.at[part(c, 1 - t)], RS.at[c], sib_s.at[c], sib_r.at[c], s_dev)))

    def mix_pair(c):
        sib[c].wait_recv()
        BR[role, c] = (MP[part(c, t), :].astype(F32) + RS[c].astype(F32)).astype(BF16)
        zc.extend(start(remote(BR.at[role, c], BR.at[role, c], z_s.at[c], z_r.at[c], z_dev)))

    def stream_chunk(c):
        zc[c].wait_recv()
        step_rows = 32

        def body(i, _):
            rows = pl.ds(pl.multiple_of(i * step_rows, step_rows), step_rows)
            mine = pl.ds(pl.multiple_of((2 * c + t) * half + i * step_rows, step_rows), step_rows)
            branch = jnp.concatenate(
                [BR[q, c, rows, s * mcols:(s + 1) * mcols] for s in range(n_fs) for q in range(2)], axis=1
            )
            stream = tok[mine, :].astype(F32) + branch.astype(F32)
            n2[mine, :] = rms_scale(stream, ffn_gain[...]).astype(BF16)
            return 0

        lax.fori_loop(0, half // step_rows, body, 0)
        ref = n2.at[part(c, t)]
        nb.extend(start(remote(ref, ref, n_s.at[c], n_r.at[c], s_dev)))

    def ffn_rows(k, i):
        _, _, _, c0, nc, _ = pieces[k]
        cuts = 2 if nc == 2 * LANES else 1
        n = 4 * half // cuts
        for a in range(c0, c0 + nc, 2 * LANES):
            w = WG[:, :, a:a + 2 * LANES].reshape(width, 2 * LANES)
            for j in range(cuts):
                rows = pl.ds(4 * i * half + j * n, n)
                zz = jnp.dot(n2[rows, :], w, preferred_element_type=F32)
                g, u = zz[:, :LANES], zz[:, LANES:]
                hidden[rows, a // 2:a // 2 + LANES] = (g / (1.0 + jnp.exp(-g)) * u).astype(BF16)

    dn = range(len(pieces) - 3, len(pieces))
    cuts = [pieces[k][3:5] for k in dn]
    groups = [
        ((f,), (0, cols)), ((x_of, y_of), cuts[0]), ((x_of, y_of), cuts[1]), ((d_of,), cuts[0]),
        ((x_of, y_of), cuts[2]), ((d_of,), cuts[1]), ((d_of,), cuts[2]),
    ]
    so, qo, written = {}, {}, []

    def down_send(k, *hs):
        slots, (c0, nc) = groups[k]
        cs = pl.ds(c0, nc)
        w = jnp.concatenate([WD[s, :hid, c0:c0 + nc] for s in slots], axis=1)
        for h in hs:
            prod = jnp.dot(
                hidden[pl.ds(4 * h * half, 4 * half), :hid], w, preferred_element_type=F32
            ).astype(BF16)
            for j, s in enumerate(slots):
                for e in range(4):
                    OP[s, e % 2, 2 * h + e // 2, :, c0:c0 + nc] = prod[e * half:(e + 1) * half, j * nc:(j + 1) * nc]
        for h in hs:
            two = pl.ds(2 * h, 2)
            so[k, h] = start(*[
                remote(
                    OP.at[s, 1 - t, two, :, cs], RO.at[s, two, :, cs], o_s.at[k, h, j], o_r.at[k, h, j], s_dev
                )
                for j, s in enumerate(slots)
            ])

    def down_pair(k, *hs):
        slots, (c0, nc) = groups[k]
        cs = pl.ds(c0, nc)
        for h in hs:
            c = 2 * h + 1 - p
            qo[k, h] = []
            for j, s in enumerate(slots):
                so[k, h][j].wait_recv()
                ZC[s, h, :, cs] = (OP[s, t, c, :, cs].astype(F32) + RO[s, c, :, cs].astype(F32)).astype(BF16)
                qo[k, h] += start(remote(
                    ZC.at[s, h, :, cs], RF.at[s, h, :, cs], q_s.at[k, h, j], q_r.at[k, h, j], z_dev
                ))

    def finish(k, h):
        slots, (c0, nc) = groups[k]
        c = 2 * h + p
        rows = pl.ds(h * half, half)
        for j, s in enumerate(slots):
            qo[k, h][j].wait_recv()
            for a in range(0, nc, LANES):
                lo = c0 + a
                q, at = lo // mcols, lo % mcols
                cs = pl.ds(lo, LANES)
                ms = pl.ds(pl.multiple_of(s * mcols + at, LANES), LANES)
                whole = pl.ds(pl.multiple_of(s * cols + lo, LANES), LANES)
                stream = tok[part(c, t), whole].astype(F32) + BR[q, c, :, ms].astype(F32)
                branch = (
                    OP[s, t, c, :, cs].astype(F32)
                    + RO[s, c, :, cs].astype(F32)
                    + RF[s, h, :, cs].astype(F32)
                )
                out[rows, whole] = (stream + branch).astype(BF16)
            block = pl.ds(pl.multiple_of(s * cols + c0, LANES), nc)
            w = pltpu.make_async_copy(out.at[rows, block], out_hbm.at[rows, block], w_s.at[k, h, j])
            w.start()
            written.append(w)

    def later(*cs):
        for c in cs:
            nb[c].wait_recv()

    if role:
        mix_in(0)
        mix_in(1)
        mix_in(2)
        step(4, 6)
        mix_in(3)
        arrived(2, 3)
        mix_out(0)
        mix_out(1)
        mix_pair(0)
        step(5, 7)
        mix_out(2)
        mix_pair(1)
        across(4)
        mix_out(3)
        mix_pair(2)
        mix_pair(3)
        step(6, 8)
        stream_chunk(0)
        across(5)
        stream_chunk(1)
        step(7)
        later(0, 1)
        arrived(4)
        ffn_rows(4, 0)
        across(6)
        arrived(5)
        ffn_rows(5, 0)
        stream_chunk(2)
        step(8, 9, 10)
        across(7)
        stream_chunk(3)
        later(2, 3)
        arrived(6)
        ffn_rows(6, 0)
        across(8)
        ffn_rows(4, 1)
        arrived(7)
        ffn_rows(7, 0)
        arrived(8)
        ffn_rows(8, 0)
        down_send(0, 0)
        ffn_rows(5, 1)
        down_pair(0, 0)
        ffn_rows(6, 1)
        step(9, 11)
        ffn_rows(7, 1)
        ffn_rows(8, 1)
        down_send(0, 1)
        step(10)
        down_pair(0, 1)
    else:
        mix_in(0)
        mix_in(1)
        step(2)
        mix_in(2)
        mix_in(3)
        step(3, 4, 5)
        arrived(2, 3)
        mix_out(0)
        mix_out(1)
        mix_pair(0)
        mix_out(2)
        mix_pair(1)
        step(4, 6)
        mix_out(3)
        mix_pair(2)
        mix_pair(3)
        stream_chunk(0)
        step(5, 7)
        stream_chunk(1)
        later(0, 1)
        arrived(4)
        ffn_rows(4, 0)
        step(6)
        stream_chunk(2)
        arrived(5)
        ffn_rows(5, 0)
        step(7, 8, 9)
        stream_chunk(3)
        later(2, 3)
        ffn_rows(4, 1)
        ffn_rows(5, 1)
        arrived(6)
        ffn_rows(6, 0)
        ffn_rows(6, 1)
        arrived(7)
        ffn_rows(7, 0)
        down_send(0, 0)
        ffn_rows(7, 1)
        down_pair(0, 0)
        down_send(0, 1)
        step(8, 10)
        down_pair(0, 1)
        step(9)

    sides(dn[0])
    down_send(1, 0, 1)
    down_pair(1, 0, 1)
    if role:
        across(dn[0])
    else:
        step(dn[2])
    sides(dn[1])
    down_send(2, 0, 1)
    down_pair(2, 0, 1)
    if role:
        step(dn[2])
    corner(dn[0])
    down_send(3, 0, 1)
    across(dn[1])
    down_pair(3, 0, 1)
    sides(dn[2])
    down_send(4, 0, 1)
    finish(0, 0)
    down_pair(4, 0, 1)
    across(dn[2])
    corner(dn[1])
    down_send(5, 0, 1)
    finish(0, 1)
    down_pair(5, 0, 1)
    corner(dn[2])
    down_send(6, 0, 1)
    finish(1, 0)
    down_pair(6, 0, 1)
    finish(1, 1)
    for k in range(2, 7):
        finish(k, 0)
        finish(k, 1)
    for c in sent:
        c.wait_send()
    for c in written:
        c.wait()


def paired_local(
    tokens, mix_gain, w_gate_b, w_gate_c, w_conv_in, conv_taps, w_mix_out, ffn_gain,
    w_ffn_gate, w_ffn_up, w_ffn_down,
):
    chip_rows, width = tokens.shape
    n_fs = lax.axis_size("fs")
    rows_d = w_gate_b.shape[0]
    ch = w_gate_b.shape[1] // 2
    units = inner_units(w_ffn_gate.shape[1])
    hid = units * LANES
    cols = w_mix_out.shape[1]
    half = chip_rows // 4
    group = 2 * chip_rows
    n_loads = 15 + 2 * units

    def vmem(*shape):
        return pltpu.VMEM(shape, BF16)

    def dma(*shape):
        return pltpu.SemaphoreType.DMA(shape)

    return pl.pallas_call(
        layer_kernel,
        out_shape=jax.ShapeDtypeStruct((2 * half, width), BF16),
        in_specs=[pl.BlockSpec(memory_space=pl.ANY)] * 11,
        out_specs=pl.BlockSpec(memory_space=pl.ANY),
        scratch_shapes=[
            vmem(2 * half, width),
            vmem(group, width),
            vmem(group, width),
            vmem(group, width),
            vmem(n_fs, rows_d, 3 * ch),
            vmem(n_fs, 2 * ch, cols // 2),
            vmem(n_fs, rows_d, 2 * hid),
            vmem(n_fs, hid, cols),
            vmem(2, group, ch),
            vmem(group, width // 2),
            vmem(N_CHUNKS, half, width // 2),
            vmem(2, N_CHUNKS, half, width // 2),
            vmem(group, hid),
            vmem(n_fs, 2, N_CHUNKS, half, cols),
            vmem(n_fs, N_CHUNKS, half, cols),
            vmem(n_fs, 2, half, cols),
            vmem(n_fs, 2, half, cols),
            pltpu.VMEM((1, width), F32),
            pltpu.VMEM(conv_taps.shape, F32),
            pltpu.VMEM((1, width), F32),
            dma(n_loads),
            *[dma(N_PIECES, 2)] * 4,
            *[dma(N_PIECES, 3)] * 2,
            *[dma(2)] * 4,
            *[dma(N_CHUNKS)] * 8,
            *[dma(7, 2, 2)] * 5,
        ],
        compiler_params=pltpu.CompilerParams(
            collective_id=0, has_side_effects=True, vmem_limit_bytes=60 * 2**20
        ),
    )(
        tokens, w_gate_b, w_gate_c, w_conv_in, w_mix_out, w_ffn_gate, w_ffn_up, w_ffn_down,
        mix_gain.reshape(1, width), conv_taps, ffn_gain.reshape(1, width),
    )


def causal_mix(product_in, conv_taps):
    shaped = product_in.reshape(product_in.shape[0] // LEN, LEN, product_in.shape[1])
    padded = jnp.pad(shaped, ((0, 0), (2, 0), (0, 0)))
    convolved = (
        conv_taps[0] * padded[:, :-2]
        + conv_taps[1] * padded[:, 1:-1]
        + conv_taps[2] * padded[:, 2:]
    )
    return convolved.reshape(product_in.shape)


def general_local(
    tokens, mix_gain, w_gate_b, w_gate_c, w_conv_in, conv_taps, w_mix_out, ffn_gain,
    w_ffn_gate, w_ffn_up, w_ffn_down,
):
    def scatter(product):
        return lax.psum_scatter(
            product.astype(BF16), "tp", scatter_dimension=0, tiled=True
        ).astype(F32)

    def dot(a, b):
        return jnp.dot(a, b, preferred_element_type=F32)

    def rows(w):
        return lax.all_gather(w, "fs", axis=0, tiled=True)

    normed = rms_scale(tokens.astype(F32), mix_gain).astype(BF16)
    gate_b, gate_c, conv_in = (dot(normed, rows(w)) for w in (w_gate_b, w_gate_c, w_conv_in))
    gated = (gate_b * causal_mix(gate_c * conv_in, conv_taps)).astype(BF16)
    row_count = normed.shape[0] // lax.axis_size("tp")
    branch = scatter(dot(gated, lax.all_gather(w_mix_out, "fs", axis=1, tiled=True)))
    own = lax.dynamic_slice_in_dim(tokens, lax.axis_index("tp") * row_count, row_count, 0)
    stream = own.astype(F32) + branch
    normed_two = lax.all_gather(
        rms_scale(stream, ffn_gain).astype(BF16), "tp", axis=0, tiled=True
    )
    hidden = (jax.nn.silu(dot(normed_two, rows(w_ffn_gate))) * dot(normed_two, rows(w_ffn_up))).astype(BF16)
    ffn_branch = scatter(dot(hidden, lax.all_gather(w_ffn_down, "fs", axis=1, tiled=True)))
    return (stream + ffn_branch).astype(BF16)


def solution(mesh):
    in_specs = (
        P(("rep", "fs"), None),
        P(),
        P("fs", "tp"),
        P("fs", "tp"),
        P("fs", "tp"),
        P(None, "tp"),
        P("tp", "fs"),
        P(),
        P("fs", "tp"),
        P("fs", "tp"),
        P("tp", "fs"),
    )
    out_specs = P(("rep", "fs", "tp"), None)
    size = mesh.shape
    square = size["tp"] == 2 and size["fs"] == 4 and size["rep"] == 4

    def local(*arrays):
        rows, width = arrays[0].shape
        channels, hidden = arrays[2].shape[1], arrays[8].shape[1]
        fits = (
            square
            and rows % (4 * LEN) == 0
            and channels % (2 * LANES) == 0
            and hidden % LANES == 0
            and hidden >= 11 * LANES
            and width % (16 * LANES) == 0
        )
        return (paired_local if fits else general_local)(*arrays)

    return jax.shard_map(local, mesh=mesh, in_specs=in_specs, out_specs=out_specs, check_vma=False)
```

```python
import jax
import jax.numpy as jnp
from jax import lax
from jax.experimental import pallas as pl
from jax.experimental.pallas import tpu as pltpu
from jax.sharding import PartitionSpec as P

LEN = 128
LANES = 128
EPSILON = 1e-06
MESH = pl.DeviceIdType.MESH
F32 = jnp.float32
BF16 = jnp.bfloat16


def rms_scale(values, gain):
    return values * lax.rsqrt(jnp.mean(values * values, axis=-1, keepdims=True) + EPSILON) * gain


N_CHUNKS = 4
TILE = 16


def inner_units(hidden):
    units = hidden // LANES
    return (7 * units + 5) // 11


def tiles(rows, share):
    return int(rows * share) // TILE * TILE


def weight_pieces(role, rows_d, n_conv, mix_rows, n_mix, units, hid, n_down):
    pieces = [(0, i * rows_d // 2, rows_d // 2, 0, n_conv, 0.375) for i in range(2)]
    pieces += [(1, i * mix_rows // 2, mix_rows // 2, 0, n_mix, 0.375) for i in range(2)]
    cuts = [i * units // 4 for i in range(4)] + [units]
    if role:
        cuts = [(u * units + 6) // 7 for u in (0, 1, 3, 5, 6)] + [units]
    pieces += [(2, 0, rows_d, 2 * LANES * a, 2 * LANES * (b - a), 0.32) for a, b in zip(cuts, cuts[1:])]
    down = (0, n_down // 2, 3 * n_down // 4, n_down)
    for a, b, share in zip(down, down[1:], (0, 0.25, 0.2)):
        pieces.append((3, 0, hid, a, b - a, share))
    return pieces


N_PIECES = 12


def layer_kernel(*refs):
    r = lax.axis_index("rep")
    p = lax.rem(r, 2)
    f = lax.axis_index("fs")
    barrier = pltpu.get_barrier_semaphore()
    x_of = f + 1 - 2 * lax.rem(f, 2)
    for dev in (
        {"fs": x_of}, {"fs": lax.rem(f + 2, 4)}, {"rep": r + 1 - 2 * p}, {"tp": 1 - lax.axis_index("tp")}
    ):
        pl.semaphore_signal(barrier, inc=1, device_id=dev, device_id_type=MESH)
    inner = jnp.logical_or(r == 1, r == 2)

    @pl.when(inner)
    def _():
        layer_body(1, barrier, *refs)

    @pl.when(jnp.logical_not(inner))
    def _():
        layer_body(0, barrier, *refs)


def layer_body(
    role, barrier,
    tokens, wb, wc, wi, wm_in, wg_in, wu_in, wd_in, mix_gain_in, taps_in, ffn_gain_in,
    out_hbm,
    out, tok, normed, n2, WA, WM, WG, WD, gated, MP, RS, BR, hidden, OP, RO, ZC, RF, mix_gain, taps, ffn_gain,
    load_sem, gone, dr, fr, ur, cr, tz_r, ts_r, g_r, sib_r, z_r, n_r, o_r, q_r,
):
    n_fs, rows_d, _ = WA.shape
    ch = gated.shape[2]
    width = tokens.shape[1]
    half = tokens.shape[0] // 4
    cols = WD.shape[2]
    mcols = WM.shape[2]
    all_units = wg_in.shape[1] // LANES
    units = inner_units(wg_in.shape[1])
    first = 0
    if not role:
        first, units = units, all_units - units
    hid = units * LANES

    r = lax.axis_index("rep")
    f = lax.axis_index("fs")
    t = lax.axis_index("tp")
    p = lax.rem(r, 2)
    twin = r - 1
    z_dev = {"rep": r + 1 - 2 * p}
    w_dev = {"rep": 3 - r}
    x_of = f + 1 - 2 * lax.rem(f, 2)
    y_of = lax.rem(f + 2, 4)
    d_of = lax.rem(x_of + 2, 4)
    x_dev, y_dev, s_dev = {"fs": x_of}, {"fs": y_of}, {"tp": 1 - t}

    def part(c, core):
        return pl.ds(pl.multiple_of((2 * c + core) * half, half), half)

    def chunk(c):
        return pl.ds(pl.multiple_of(2 * c * half, 2 * half), 2 * half)

    if role:
        pl.semaphore_signal(barrier, inc=1, device_id=w_dev, device_id_type=MESH)

    chan = pl.ds(role * ch, ch)
    def load(src, dst, k):
        pltpu.make_async_copy(src, dst, load_sem.at[k]).start()

    def loaded(ref, k):
        pltpu.make_async_copy(ref, ref, load_sem.at[k]).wait()

    w_rows = [pl.ds(k * (rows_d // 2), rows_d // 2) for k in range(2)]
    for k in range(2):
        for i, w in enumerate((wb, wc, wi)):
            load(w.at[w_rows[k], chan], WA.at[f, w_rows[k], pl.ds(i * ch, ch)], k)
    for h in range(2):
        for core in range(2):
            load(tokens.at[pl.ds((2 * core + h) * half, half)], tok.at[part(2 * h + p, core)], 2)
    small = ((mix_gain_in, mix_gain), (taps_in, taps), (ffn_gain_in, ffn_gain))
    for i, (src, dst) in enumerate(small):
        load(src, dst, 3 + i)
    pl.semaphore_wait(barrier, 4 + role)

    def remote(src, dst, s, rcv, dev):
        return pltpu.make_async_remote_copy(
            src_ref=src, dst_ref=dst, send_sem=s, recv_sem=rcv, device_id=dev, device_id_type=MESH
        )

    bufs = (WA, WM, WG, WD)
    pieces = weight_pieces(role, rows_d, 3 * ch, WM.shape[1], mcols, units, hid, cols)

    def cut(k, slot, lo, n):
        w, r0, _, c0, nc, _ = pieces[k]
        at = r0 + lo
        if not isinstance(at, int):
            at = pl.multiple_of(at, TILE)
        return bufs[w].at[slot, pl.ds(at, n), pl.ds(c0, nc)]

    def share(k):
        rows = pieces[k][2]
        lent = tiles(rows, pieces[k][5]) if role else 0
        kept = rows - lent
        near = tiles(kept, 0.5)
        lo = twin * lent if role else 0
        mine = twin * kept if role else 0
        return lent, kept, near, lo, mine

    def direct(k):
        _, kept, _, lo, _ = share(k)
        ref = cut(k, f, lo, kept)
        sem = gone.at[pieces[k][0]]
        return [remote(ref, ref, sem, dr.at[k], dev) for dev in (x_dev, y_dev)]

    def forward(k):
        _, kept, near, lo, _ = share(k)
        a, b = cut(k, x_of, lo, near), cut(k, y_of, lo + near, kept - near)
        return [
            remote(b, b, gone.at[pieces[k][0]], fr.at[k], x_dev),
            remote(a, a, gone.at[pieces[k][0]], fr.at[k], y_dev),
        ]

    def lend(k, sems, *slots):
        lent, _, _, _, mine = share(k)
        if not lent:
            return []
        refs = [cut(k, slot, mine, lent) for slot in slots]
        return [remote(ref, ref, gone.at[pieces[k][0]], sems.at[k], w_dev) for ref in refs]

    def start(*copies):
        for c in copies:
            c.start()

    def landed(ref, sem):
        remote(ref, ref, sem, sem, s_dev).wait_recv()

    def left(ref, k):
        remote(ref, ref, gone.at[k], gone.at[k], s_dev).wait_send()

    passed = set()

    def send(*ks):
        for k in ks:
            start(*direct(k))

    def step(k, *more):
        landed(cut(k, pl.ds(0, 2), 0, share(k)[1]), dr.at[k])
        start(*forward(k))
        if role:
            start(*lend(k, ur, x_of, y_of))
        send(*more)

    def across(*ks):
        for k in ks:
            if k not in passed:
                passed.add(k)
                landed(cut(k, 0, 0, share(k)[1]), fr.at[k])
                if role:
                    start(*lend(k, cr, d_of))

    def sides(*ks):
        for k in ks:
            if share(k)[0]:
                landed(cut(k, pl.ds(0, 2), 0, share(k)[0]), ur.at[k])

    def corner(*ks):
        across(*ks)
        for k in ks:
            if share(k)[0]:
                landed(cut(k, 0, 0, share(k)[0]), cr.at[k])

    def arrived(*ks):
        across(*ks)
        sides(*ks)
        corner(*ks)

    for k in range(2):
        loaded(WA.at[f, w_rows[k]], k)
        send(k)
    loaded(tok.at[pl.ds(0, 4 * half)], 2)
    for i, (_, dst) in enumerate(small):
        loaded(dst, 3 + i)
    for h in range(2):
        ref = tok.at[part(2 * h + p, t)]
        start(remote(ref, ref, gone.at[4], tz_r.at[h], z_dev))

    def relay(h):
        ref = tok.at[part(2 * h + 1 - p, t)]
        landed(ref, tz_r.at[h])
        start(remote(ref, ref, gone.at[5], ts_r.at[h], s_dev))

    def sibling(h):
        landed(tok.at[part(2 * h, t)], ts_r.at[h])

    def norm_chunk(c):
        def body(i, _):
            rows = pl.ds(pl.multiple_of(2 * c * half + i * 64, 64), 64)
            normed[rows, :] = rms_scale(tok[rows, :].astype(F32), mix_gain[...]).astype(BF16)
            return 0

        lax.fori_loop(0, 2 * half // 64, body, 0)

    load(wm_in.at[:, pl.ds(role * mcols, mcols)], WM.at[f], 6)
    for c in range(units):
        for i, w in enumerate((wg_in, wu_in)):
            load(w.at[:, pl.ds((first + c) * LANES, LANES)], WG.at[f, :, pl.ds((2 * c + i) * LANES, LANES)], 7)
    load(wd_in.at[pl.ds(first * LANES, hid)], WD.at[f, pl.ds(0, hid)], 8)

    norm_chunk(p)
    norm_chunk(2 + p)
    loaded(WM.at[f], 6)
    loaded(WG.at[f, :, pl.ds(0, 2 * hid)], 7)
    loaded(WD.at[f, pl.ds(0, hid)], 8)
    step(0)
    relay(0)
    if role:
        step(1, 2, 3)
        sibling(0)
        norm_chunk(1 - p)
        across(0)
        across(1)
        step(2)
        step(3, 4, 5)
        relay(1)
        sibling(1)
        norm_chunk(3 - p)
        across(2)
        across(3)
    else:
        sibling(0)
        norm_chunk(1 - p)
        step(1, 2, 3)
        relay(1)
        sibling(1)
        norm_chunk(3 - p)
    arrived(0, 1)

    tap = [taps[pl.ds(i, 1), chan] for i in range(3)]
    pos = lax.rem(lax.broadcasted_iota(jnp.int32, (2 * half, ch), 0), LEN)

    def mix_in(c):
        x = normed[chunk(c), :]

        def proj(q):
            w = WA[:, :, q * ch:(q + 1) * ch].reshape(width, ch)
            return jnp.dot(x, w, preferred_element_type=F32)

        pr = proj(1) * proj(2)
        one = jnp.where(pos >= 1, pltpu.roll(pr, 1, 0), 0.0)
        two = jnp.where(pos >= 2, pltpu.roll(pr, 2, 0), 0.0)
        conv = tap[0] * two + tap[1] * one + tap[2] * pr
        gated[role, chunk(c), :] = (proj(0) * conv).astype(BF16)
        ref = gated.at[role, chunk(c)]
        start(remote(ref, ref, gone.at[6], g_r.at[c], z_dev))

    def mix_out(c):
        landed(gated.at[role, chunk(c)], g_r.at[c])
        g = jnp.concatenate([gated[0, chunk(c), :], gated[1, chunk(c), :]], axis=1)
        for s in range(n_fs):
            MP[chunk(c), s * mcols:(s + 1) * mcols] = jnp.dot(
                g, WM[s], preferred_element_type=F32
            ).astype(BF16)
        start(remote(MP.at[part(c, 1 - t)], RS.at[c], gone.at[7], sib_r.at[c], s_dev))

    def mix_pair(c):
        landed(RS.at[c], sib_r.at[c])
        BR[role, c] = (MP[part(c, t), :].astype(F32) + RS[c].astype(F32)).astype(BF16)
        start(remote(BR.at[role, c], BR.at[role, c], gone.at[8], z_r.at[c], z_dev))

    def stream_chunk(c):
        landed(BR.at[1 - role, c], z_r.at[c])
        step_rows = 32

        def body(i, _):
            rows = pl.ds(pl.multiple_of(i * step_rows, step_rows), step_rows)
            mine = pl.ds(pl.multiple_of((2 * c + t) * half + i * step_rows, step_rows), step_rows)
            branch = jnp.concatenate(
                [BR[q, c, rows, s * mcols:(s + 1) * mcols] for s in range(n_fs) for q in range(2)], axis=1
            )
            stream = tok[mine, :].astype(F32) + branch.astype(F32)
            n2[mine, :] = rms_scale(stream, ffn_gain[...]).astype(BF16)
            return 0

        lax.fori_loop(0, half // step_rows, body, 0)
        ref = n2.at[part(c, t)]
        start(remote(ref, ref, gone.at[9], n_r.at[c], s_dev))

    def ffn_rows(k, i):
        _, _, _, c0, nc, _ = pieces[k]
        cuts = 2 if nc == 2 * LANES else 1
        n = 4 * half // cuts
        for a in range(c0, c0 + nc, 2 * LANES):
            w = WG[:, :, a:a + 2 * LANES].reshape(width, 2 * LANES)
            for j in range(cuts):
                rows = pl.ds(4 * i * half + j * n, n)
                zz = jnp.dot(n2[rows, :], w, preferred_element_type=F32)
                g, u = zz[:, :LANES], zz[:, LANES:]
                hidden[rows, a // 2:a // 2 + LANES] = (g / (1.0 + jnp.exp(-g)) * u).astype(BF16)

    dn = range(len(pieces) - 3, len(pieces))
    cuts = [pieces[k][3:5] for k in dn]
    groups = [
        ((f,), (0, cols)), ((x_of, y_of), cuts[0]), ((x_of, y_of), cuts[1]), ((d_of,), cuts[0]),
        ((x_of, y_of), cuts[2]), ((d_of,), cuts[1]), ((d_of,), cuts[2]),
    ]
    def span(k, hs):
        n = len(groups[k][0])
        return n, pl.ds(*groups[k][1]), pl.ds(2 * hs[0], 2 * len(hs)), pl.ds(hs[0], len(hs)), 7 * hs[0] + k

    def down_send(k, *hs):
        slots, (c0, nc) = groups[k]
        _, cs, two, _, sem = span(k, hs)
        w = jnp.concatenate([WD[s, :hid, c0:c0 + nc] for s in slots], axis=1)
        for h in hs:
            prod = jnp.dot(
                hidden[pl.ds(4 * h * half, 4 * half), :hid], w, preferred_element_type=F32
            ).astype(BF16)
            for j, s in enumerate(slots):
                for e in range(4):
                    OP[s, e % 2, 2 * h + e // 2, :, c0:c0 + nc] = prod[e * half:(e + 1) * half, j * nc:(j + 1) * nc]
        for s in slots:
            start(remote(OP.at[s, 1 - t, two, :, cs], RO.at[s, two, :, cs], gone.at[10], o_r.at[sem], s_dev))

    def down_pair(k, *hs):
        slots, _ = groups[k]
        n, cs, two, rows, sem = span(k, hs)
        landed(RO.at[pl.ds(0, n), two, :, cs], o_r.at[sem])
        for s in slots:
            for h in hs:
                c = 2 * h + 1 - p
                ZC[s, h, :, cs] = (OP[s, t, c, :, cs].astype(F32) + RO[s, c, :, cs].astype(F32)).astype(BF16)
            start(remote(ZC.at[s, rows, :, cs], RF.at[s, rows, :, cs], gone.at[11], q_r.at[sem], z_dev))

    def finish(k, *hs):
        slots, (c0, nc) = groups[k]
        n, cs, _, rows, sem = span(k, hs)
        landed(RF.at[pl.ds(0, n), rows, :, cs], q_r.at[sem])
        for s in slots:
            for h in hs:
                c = 2 * h + p
                for a in range(0, nc, LANES):
                    lo = c0 + a
                    q, at = lo // mcols, lo % mcols
                    cs = pl.ds(lo, LANES)
                    ms = pl.ds(pl.multiple_of(s * mcols + at, LANES), LANES)
                    whole = pl.ds(pl.multiple_of(s * cols + lo, LANES), LANES)
                    stream = tok[part(c, t), whole].astype(F32) + BR[q, c, :, ms].astype(F32)
                    branch = (
                        OP[s, t, c, :, cs].astype(F32)
                        + RO[s, c, :, cs].astype(F32)
                        + RF[s, h, :, cs].astype(F32)
                    )
                    out[h * half:(h + 1) * half, whole] = (stream + branch).astype(BF16)
            lines = pl.ds(hs[0] * half, len(hs) * half)
            block = pl.ds(pl.multiple_of(s * cols + c0, LANES), nc)
            pltpu.make_async_copy(out.at[lines, block], out_hbm.at[lines, block], load_sem.at[9]).start()

    def later(*cs):
        for c in cs:
            landed(n2.at[part(c, 1 - t)], n_r.at[c])

    if role:
        mix_in(0)
        mix_in(1)
        mix_in(2)
        step(4, 6)
        mix_in(3)
        arrived(2, 3)
        mix_out(0)
        mix_out(1)
        mix_pair(0)
        step(5, 7)
        mix_out(2)
        mix_pair(1)
        across(4)
        mix_out(3)
        mix_pair(2)
        mix_pair(3)
        step(6, 8)
        stream_chunk(0)
        across(5)
        stream_chunk(1)
        step(7)
        later(0, 1)
        arrived(4)
        ffn_rows(4, 0)
        across(6)
        arrived(5)
        ffn_rows(5, 0)
        stream_chunk(2)
        step(8, 9, 10, 11)
        across(7)
        stream_chunk(3)
        later(2, 3)
        arrived(6)
        ffn_rows(6, 0)
        across(8)
        ffn_rows(4, 1)
        arrived(7)
        ffn_rows(7, 0)
        arrived(8)
        ffn_rows(8, 0)
        down_send(0, 0)
        ffn_rows(5, 1)
        down_pair(0, 0)
        ffn_rows(6, 1)
        step(9)
        ffn_rows(7, 1)
        ffn_rows(8, 1)
        down_send(0, 1)
        step(10)
        down_pair(0, 1)
    else:
        mix_in(0)
        mix_in(1)
        step(2)
        mix_in(2)
        mix_in(3)
        step(3, 4, 5)
        arrived(2, 3)
        mix_out(0)
        mix_out(1)
        mix_pair(0)
        mix_out(2)
        mix_pair(1)
        step(4, 6)
        mix_out(3)
        mix_pair(2)
        mix_pair(3)
        stream_chunk(0)
        step(5, 7)
        stream_chunk(1)
        later(0, 1)
        arrived(4)
        ffn_rows(4, 0)
        step(6)
        stream_chunk(2)
        arrived(5)
        ffn_rows(5, 0)
        step(7, 8, 9)
        stream_chunk(3)
        later(2, 3)
        ffn_rows(4, 1)
        ffn_rows(5, 1)
        arrived(6)
        ffn_rows(6, 0)
        ffn_rows(6, 1)
        arrived(7)
        ffn_rows(7, 0)
        down_send(0, 0)
        ffn_rows(7, 1)
        down_pair(0, 0)
        down_send(0, 1)
        step(8, 10)
        down_pair(0, 1)
        step(9)

    sides(dn[0])
    down_send(1, 0, 1)
    down_pair(1, 0, 1)
    if role:
        step(dn[2])
    sides(dn[1])
    down_send(2, 0, 1)
    down_pair(2, 0, 1)
    across(dn[0])
    if not role:
        step(dn[2])
    finish(0, 0)
    sides(dn[2])
    down_send(4, 0, 1)
    down_pair(4, 0, 1)
    corner(dn[0])
    down_send(3, 0, 1)
    finish(0, 1)
    across(dn[1])
    down_pair(3, 0, 1)
    corner(dn[1])
    down_send(5, 0, 1)
    across(dn[2])
    down_pair(5, 0, 1)
    corner(dn[2])
    down_send(6, 0, 1)
    finish(1, 0, 1)
    down_pair(6, 0, 1)
    for k in (2, 4, 3, 5, 6):
        finish(k, 0, 1)
    for w, ref in enumerate((
        WA.at[pl.ds(0, 3)], WM.at[pl.ds(0, 3)], WG.at[pl.ds(0, 3), :, pl.ds(0, 2 * hid)],
        WD.at[pl.ds(0, 3), pl.ds(0, hid)], tok.at[pl.ds(0, 2 * half)], tok.at[pl.ds(0, 2 * half)],
        gated.at[role], RS, BR.at[role], n2.at[pl.ds(0, 4 * half)], RO, ZC,
    )):
        left(ref, w)
    loaded(out, 9)


def paired_local(
    tokens, mix_gain, w_gate_b, w_gate_c, w_conv_in, conv_taps, w_mix_out, ffn_gain,
    w_ffn_gate, w_ffn_up, w_ffn_down,
):
    chip_rows, width = tokens.shape
    n_fs = lax.axis_size("fs")
    rows_d = w_gate_b.shape[0]
    ch = w_gate_b.shape[1] // 2
    units = inner_units(w_ffn_gate.shape[1])
    hid = units * LANES
    cols = w_mix_out.shape[1]
    half = chip_rows // 4
    group = 2 * chip_rows

    def vmem(*shape):
        return pltpu.VMEM(shape, BF16)

    def dma(*shape):
        return pltpu.SemaphoreType.DMA(shape)

    return pl.pallas_call(
        layer_kernel,
        out_shape=jax.ShapeDtypeStruct((2 * half, width), BF16),
        in_specs=[pl.BlockSpec(memory_space=pl.ANY)] * 11,
        out_specs=pl.BlockSpec(memory_space=pl.ANY),
        scratch_shapes=[
            vmem(2 * half, width),
            vmem(group, width),
            vmem(group, width),
            vmem(group, width),
            vmem(n_fs, rows_d, 3 * ch),
            vmem(n_fs, 2 * ch, cols // 2),
            vmem(n_fs, rows_d, 2 * hid),
            vmem(n_fs, hid, cols),
            vmem(2, group, ch),
            vmem(group, width // 2),
            vmem(N_CHUNKS, half, width // 2),
            vmem(2, N_CHUNKS, half, width // 2),
            vmem(group, hid),
            vmem(n_fs, 2, N_CHUNKS, half, cols),
            vmem(n_fs, N_CHUNKS, half, cols),
            vmem(n_fs, 2, half, cols),
            vmem(n_fs, 2, half, cols),
            pltpu.VMEM((1, width), F32),
            pltpu.VMEM(conv_taps.shape, F32),
            pltpu.VMEM((1, width), F32),
            dma(10),
            dma(12),
            *[dma(N_PIECES)] * 4,
            *[dma(2)] * 2,
            *[dma(N_CHUNKS)] * 4,
            *[dma(14)] * 2,
        ],
        compiler_params=pltpu.CompilerParams(
            collective_id=0, has_side_effects=True, vmem_limit_bytes=60 * 2**20
        ),
    )(
        tokens, w_gate_b, w_gate_c, w_conv_in, w_mix_out, w_ffn_gate, w_ffn_up, w_ffn_down,
        mix_gain.reshape(1, width), conv_taps, ffn_gain.reshape(1, width),
    )


def causal_mix(product_in, conv_taps):
    shaped = product_in.reshape(product_in.shape[0] // LEN, LEN, product_in.shape[1])
    padded = jnp.pad(shaped, ((0, 0), (2, 0), (0, 0)))
    convolved = (
        conv_taps[0] * padded[:, :-2]
        + conv_taps[1] * padded[:, 1:-1]
        + conv_taps[2] * padded[:, 2:]
    )
    return convolved.reshape(product_in.shape)


def general_local(
    tokens, mix_gain, w_gate_b, w_gate_c, w_conv_in, conv_taps, w_mix_out, ffn_gain,
    w_ffn_gate, w_ffn_up, w_ffn_down,
):
    def scatter(product):
        return lax.psum_scatter(
            product.astype(BF16), "tp", scatter_dimension=0, tiled=True
        ).astype(F32)

    def dot(a, b):
        return jnp.dot(a, b, preferred_element_type=F32)

    def rows(w):
        return lax.all_gather(w, "fs", axis=0, tiled=True)

    normed = rms_scale(tokens.astype(F32), mix_gain).astype(BF16)
    gate_b, gate_c, conv_in = (dot(normed, rows(w)) for w in (w_gate_b, w_gate_c, w_conv_in))
    gated = (gate_b * causal_mix(gate_c * conv_in, conv_taps)).astype(BF16)
    row_count = normed.shape[0] // lax.axis_size("tp")
    branch = scatter(dot(gated, lax.all_gather(w_mix_out, "fs", axis=1, tiled=True)))
    own = lax.dynamic_slice_in_dim(tokens, lax.axis_index("tp") * row_count, row_count, 0)
    stream = own.astype(F32) + branch
    normed_two = lax.all_gather(
        rms_scale(stream, ffn_gain).astype(BF16), "tp", axis=0, tiled=True
    )
    hidden = (jax.nn.silu(dot(normed_two, rows(w_ffn_gate))) * dot(normed_two, rows(w_ffn_up))).astype(BF16)
    ffn_branch = scatter(dot(hidden, lax.all_gather(w_ffn_down, "fs", axis=1, tiled=True)))
    return (stream + ffn_branch).astype(BF16)


def solution(mesh):
    in_specs = (
        P(("rep", "fs"), None),
        P(),
        P("fs", "tp"),
        P("fs", "tp"),
        P("fs", "tp"),
        P(None, "tp"),
        P("tp", "fs"),
        P(),
        P("fs", "tp"),
        P("fs", "tp"),
        P("tp", "fs"),
    )
    out_specs = P(("rep", "fs", "tp"), None)
    size = mesh.shape
    square = size["tp"] == 2 and size["fs"] == 4 and size["rep"] == 4

    def local(*arrays):
        rows, width = arrays[0].shape
        channels, hidden = arrays[2].shape[1], arrays[8].shape[1]
        fits = (
            square
            and rows % (4 * LEN) == 0
            and channels % (2 * LANES) == 0
            and hidden % LANES == 0
            and hidden >= 11 * LANES
            and width % (16 * LANES) == 0
        )
        return (paired_local if fits else general_local)(*arrays)

    return jax.shard_map(local, mesh=mesh, in_specs=in_specs, out_specs=out_specs, check_vma=False)
```

```python
import jax
import jax.numpy as jnp
from jax import lax
from jax.experimental import pallas as pl
from jax.experimental.pallas import tpu as pltpu
from jax.sharding import PartitionSpec as P

LEN = 128
LANES = 128
EPSILON = 1e-06
MESH = pl.DeviceIdType.MESH
F32 = jnp.float32
BF16 = jnp.bfloat16


def rms_scale(values, gain):
    return values * lax.rsqrt(jnp.mean(values * values, axis=-1, keepdims=True) + EPSILON) * gain


N_CHUNKS = 4
TILE = 16


def inner_units(hidden):
    units = hidden // LANES
    return (7 * units + 5) // 11


def tiles(rows, share):
    return int(rows * share) // TILE * TILE


def head_rows(role, rows):
    if role:
        return [0, rows // 4, 5 * rows // 8, rows]
    return [0, rows // 2, rows]


def weight_pieces(role, rows_d, n_conv, mix_rows, n_mix, units, hid, n_down):
    starts = head_rows(role, rows_d)
    head = [(0, a, b - a, 0, n_conv, 0.375) for a, b in zip(starts, starts[1:])]
    pieces = head[:2]
    pieces += [(1, i * mix_rows // 2, mix_rows // 2, 0, n_mix, 0.375) for i in range(2)]
    cuts = [i * units // 4 for i in range(4)] + [units]
    if role:
        cuts = [(u * units + 6) // 7 for u in (0, 1, 3, 5, 6)] + [units]
    pieces += [(2, 0, rows_d, 2 * LANES * a, 2 * LANES * (b - a), 0.32) for a, b in zip(cuts, cuts[1:])]
    down = (0, n_down // 2, 3 * n_down // 4, n_down)
    for a, b, share in zip(down, down[1:], (0, 0.25, 0.2)):
        pieces.append((3, 0, hid, a, b - a, share))
    return pieces + head[2:]


N_PIECES = 13


def layer_kernel(*refs):
    r = lax.axis_index("rep")
    p = lax.rem(r, 2)
    f = lax.axis_index("fs")
    barrier = pltpu.get_barrier_semaphore()
    x_of = f + 1 - 2 * lax.rem(f, 2)
    for dev in (
        {"fs": x_of}, {"fs": lax.rem(f + 2, 4)}, {"rep": r + 1 - 2 * p}, {"tp": 1 - lax.axis_index("tp")}
    ):
        pl.semaphore_signal(barrier, inc=1, device_id=dev, device_id_type=MESH)
    inner = jnp.logical_or(r == 1, r == 2)

    @pl.when(inner)
    def _():
        layer_body(1, barrier, *refs)

    @pl.when(jnp.logical_not(inner))
    def _():
        layer_body(0, barrier, *refs)


def layer_body(
    role, barrier,
    tokens, wb, wc, wi, wm_in, wg_in, wu_in, wd_in, mix_gain_in, taps_in, ffn_gain_in,
    out,
    tok, normed, n2, WA, WM, WG, WD, gated, MP, RS, BR, hidden, OP, RO, ZC, RF, mix_gain, taps, ffn_gain,
    load_sem, gone, dr, fr, ur, cr, tz_r, ts_r, g_r, sib_r, z_r, n_r, o_r, q_r,
):
    n_fs, rows_d, _ = WA.shape
    ch = gated.shape[2]
    width = tokens.shape[1]
    half = tokens.shape[0] // 4
    cols = WD.shape[2]
    mcols = WM.shape[2]
    all_units = wg_in.shape[1] // LANES
    units = inner_units(wg_in.shape[1])
    first = 0
    if not role:
        first, units = units, all_units - units
    hid = units * LANES

    r = lax.axis_index("rep")
    f = lax.axis_index("fs")
    t = lax.axis_index("tp")
    p = lax.rem(r, 2)
    twin = r - 1
    z_dev = {"rep": r + 1 - 2 * p}
    w_dev = {"rep": 3 - r}
    x_of = f + 1 - 2 * lax.rem(f, 2)
    y_of = lax.rem(f + 2, 4)
    d_of = lax.rem(x_of + 2, 4)
    x_dev, y_dev, s_dev = {"fs": x_of}, {"fs": y_of}, {"tp": 1 - t}

    def part(c, core):
        return pl.ds(pl.multiple_of((2 * c + core) * half, half), half)

    def chunk(c):
        return pl.ds(pl.multiple_of(2 * c * half, 2 * half), 2 * half)

    if role:
        pl.semaphore_signal(barrier, inc=1, device_id=w_dev, device_id_type=MESH)

    chan = pl.ds(role * ch, ch)
    def load(src, dst, k):
        pltpu.make_async_copy(src, dst, load_sem.at[k]).start()

    def loaded(ref, k):
        pltpu.make_async_copy(ref, ref, load_sem.at[k]).wait()

    starts = head_rows(role, rows_d)
    w_rows = [pl.ds(a, b - a) for a, b in zip(starts, starts[1:])]
    for k in range(len(w_rows)):
        for i, w in enumerate((wb, wc, wi)):
            load(w.at[w_rows[k], chan], WA.at[f, w_rows[k], pl.ds(i * ch, ch)], (0, 1, 10)[k])
    for h in range(2):
        for core in range(2):
            load(tokens.at[pl.ds((2 * core + h) * half, half)], tok.at[part(2 * h + p, core)], 2)
    small = ((mix_gain_in, mix_gain), (taps_in, taps), (ffn_gain_in, ffn_gain))
    for i, (src, dst) in enumerate(small):
        load(src, dst, 3 + i)
    pl.semaphore_wait(barrier, 4 + role)

    def remote(src, dst, s, rcv, dev):
        return pltpu.make_async_remote_copy(
            src_ref=src, dst_ref=dst, send_sem=s, recv_sem=rcv, device_id=dev, device_id_type=MESH
        )

    bufs = (WA, WM, WG, WD)
    pieces = weight_pieces(role, rows_d, 3 * ch, WM.shape[1], mcols, units, hid, cols)

    def cut(k, slot, lo, n):
        w, r0, _, c0, nc, _ = pieces[k]
        at = r0 + lo
        if not isinstance(at, int):
            at = pl.multiple_of(at, TILE)
        return bufs[w].at[slot, pl.ds(at, n), pl.ds(c0, nc)]

    def share(k):
        rows = pieces[k][2]
        lent = tiles(rows, pieces[k][5]) if role else 0
        kept = rows - lent
        near = tiles(kept, 0.5)
        lo = twin * lent if role else 0
        mine = twin * kept if role else 0
        return lent, kept, near, lo, mine

    def direct(k):
        _, kept, _, lo, _ = share(k)
        ref = cut(k, f, lo, kept)
        sem = gone.at[pieces[k][0]]
        return [remote(ref, ref, sem, dr.at[k], dev) for dev in (x_dev, y_dev)]

    def forward(k):
        _, kept, near, lo, _ = share(k)
        a, b = cut(k, x_of, lo, near), cut(k, y_of, lo + near, kept - near)
        return [
            remote(b, b, gone.at[pieces[k][0]], fr.at[k], x_dev),
            remote(a, a, gone.at[pieces[k][0]], fr.at[k], y_dev),
        ]

    def lend(k, sems, *slots):
        lent, _, _, _, mine = share(k)
        if not lent:
            return []
        refs = [cut(k, slot, mine, lent) for slot in slots]
        return [remote(ref, ref, gone.at[pieces[k][0]], sems.at[k], w_dev) for ref in refs]

    def start(*copies):
        for c in copies:
            c.start()

    def landed(ref, sem):
        remote(ref, ref, sem, sem, s_dev).wait_recv()

    def left(ref, k):
        remote(ref, ref, gone.at[k], gone.at[k], s_dev).wait_send()

    passed = set()

    def send(*ks):
        for k in ks:
            start(*direct(k))

    def step(k, *more):
        landed(cut(k, pl.ds(0, 2), 0, share(k)[1]), dr.at[k])
        start(*forward(k))
        if role:
            start(*lend(k, ur, x_of, y_of))
        send(*more)

    def across(*ks):
        for k in ks:
            if k not in passed:
                passed.add(k)
                landed(cut(k, 0, 0, share(k)[1]), fr.at[k])
                if role:
                    start(*lend(k, cr, d_of))

    def sides(*ks):
        for k in ks:
            if share(k)[0]:
                landed(cut(k, pl.ds(0, 2), 0, share(k)[0]), ur.at[k])

    def corner(*ks):
        across(*ks)
        for k in ks:
            if share(k)[0]:
                landed(cut(k, 0, 0, share(k)[0]), cr.at[k])

    def arrived(*ks):
        across(*ks)
        sides(*ks)
        corner(*ks)

    for k in range(len(w_rows)):
        loaded(WA.at[f, w_rows[k]], (0, 1, 10)[k])
        send((0, 1, 12)[k])
    loaded(tok.at[pl.ds(0, 4 * half)], 2)
    for i, (_, dst) in enumerate(small):
        loaded(dst, 3 + i)
    for h in range(2):
        ref = tok.at[part(2 * h + p, t)]
        start(remote(ref, ref, gone.at[4], tz_r.at[h], z_dev))

    def relay(h):
        ref = tok.at[part(2 * h + 1 - p, t)]
        landed(ref, tz_r.at[h])
        start(remote(ref, ref, gone.at[5], ts_r.at[h], s_dev))

    def sibling(h):
        landed(tok.at[part(2 * h, t)], ts_r.at[h])

    def norm_chunk(c):
        def body(i, _):
            rows = pl.ds(pl.multiple_of(2 * c * half + i * 64, 64), 64)
            normed[rows, :] = rms_scale(tok[rows, :].astype(F32), mix_gain[...]).astype(BF16)
            return 0

        lax.fori_loop(0, 2 * half // 64, body, 0)

    load(wm_in.at[:, pl.ds(role * mcols, mcols)], WM.at[f], 6)
    for c in range(units):
        for i, w in enumerate((wg_in, wu_in)):
            load(w.at[:, pl.ds((first + c) * LANES, LANES)], WG.at[f, :, pl.ds((2 * c + i) * LANES, LANES)], 7)
    load(wd_in.at[pl.ds(first * LANES, hid)], WD.at[f, pl.ds(0, hid)], 8)

    norm_chunk(p)
    norm_chunk(2 + p)
    loaded(WM.at[f], 6)
    loaded(WG.at[f, :, pl.ds(0, 2 * hid)], 7)
    loaded(WD.at[f, pl.ds(0, hid)], 8)
    step(0)
    if role:
        step(1)
    relay(0)
    if role:
        step(12, 2, 3)
        sibling(0)
        norm_chunk(1 - p)
        across(0)
        across(1)
        across(12)
        step(2)
        step(3, 4, 5)
        relay(1)
        sibling(1)
        norm_chunk(3 - p)
        across(2)
        across(3)
    else:
        sibling(0)
        norm_chunk(1 - p)
        step(1, 2, 3)
        relay(1)
        sibling(1)
        norm_chunk(3 - p)
    arrived(0, 1, *((12,) if role else ()))

    tap = [taps[pl.ds(i, 1), chan] for i in range(3)]
    pos = lax.rem(lax.broadcasted_iota(jnp.int32, (2 * half, ch), 0), LEN)

    def mix_in(c):
        x = normed[chunk(c), :]

        def proj(q):
            w = WA[:, :, q * ch:(q + 1) * ch].reshape(width, ch)
            return jnp.dot(x, w, preferred_element_type=F32)

        pr = proj(1) * proj(2)
        one = jnp.where(pos >= 1, pltpu.roll(pr, 1, 0), 0.0)
        two = jnp.where(pos >= 2, pltpu.roll(pr, 2, 0), 0.0)
        conv = tap[0] * two + tap[1] * one + tap[2] * pr
        gated[role, chunk(c), :] = (proj(0) * conv).astype(BF16)
        ref = gated.at[role, chunk(c)]
        start(remote(ref, ref, gone.at[6], g_r.at[c], z_dev))

    def mix_out(c):
        landed(gated.at[role, chunk(c)], g_r.at[c])
        g = jnp.concatenate([gated[0, chunk(c), :], gated[1, chunk(c), :]], axis=1)
        for s in range(n_fs):
            MP[chunk(c), s * mcols:(s + 1) * mcols] = jnp.dot(
                g, WM[s], preferred_element_type=F32
            ).astype(BF16)
        start(remote(MP.at[part(c, 1 - t)], RS.at[c], gone.at[7], sib_r.at[c], s_dev))

    def mix_pair(c):
        landed(RS.at[c], sib_r.at[c])
        BR[role, c] = (MP[part(c, t), :].astype(F32) + RS[c].astype(F32)).astype(BF16)
        start(remote(BR.at[role, c], BR.at[role, c], gone.at[8], z_r.at[c], z_dev))

    def stream_chunk(c):
        landed(BR.at[1 - role, c], z_r.at[c])
        step_rows = 32

        def body(i, _):
            rows = pl.ds(pl.multiple_of(i * step_rows, step_rows), step_rows)
            mine = pl.ds(pl.multiple_of((2 * c + t) * half + i * step_rows, step_rows), step_rows)
            branch = jnp.concatenate(
                [BR[q, c, rows, s * mcols:(s + 1) * mcols] for s in range(n_fs) for q in range(2)], axis=1
            )
            stream = tok[mine, :].astype(F32) + branch.astype(F32)
            n2[mine, :] = rms_scale(stream, ffn_gain[...]).astype(BF16)
            return 0

        lax.fori_loop(0, half // step_rows, body, 0)
        ref = n2.at[part(c, t)]
        start(remote(ref, ref, gone.at[9], n_r.at[c], s_dev))

    def ffn_rows(k, i):
        _, _, _, c0, nc, _ = pieces[k]
        cuts = 2 if nc == 2 * LANES else 1
        n = 4 * half // cuts
        for a in range(c0, c0 + nc, 2 * LANES):
            w = WG[:, :, a:a + 2 * LANES].reshape(width, 2 * LANES)
            for j in range(cuts):
                rows = pl.ds(4 * i * half + j * n, n)
                zz = jnp.dot(n2[rows, :], w, preferred_element_type=F32)
                g, u = zz[:, :LANES], zz[:, LANES:]
                hidden[rows, a // 2:a // 2 + LANES] = (g / (1.0 + jnp.exp(-g)) * u).astype(BF16)

    dn = (9, 10, 11) if role else (8, 9, 10)
    cuts = [pieces[k][3:5] for k in dn]
    groups = [
        ((f,), (0, cols)), ((x_of, y_of), cuts[0]), ((x_of, y_of), cuts[1]), ((d_of,), cuts[0]),
        ((x_of, y_of), cuts[2]), ((d_of,), cuts[1]), ((d_of,), cuts[2]),
    ]
    def span(k, hs):
        n = len(groups[k][0])
        return n, pl.ds(*groups[k][1]), pl.ds(2 * hs[0], 2 * len(hs)), pl.ds(hs[0], len(hs)), 7 * hs[0] + k

    def down_send(k, *hs):
        slots, (c0, nc) = groups[k]
        _, cs, two, _, sem = span(k, hs)
        w = jnp.concatenate([WD[s, :hid, c0:c0 + nc] for s in slots], axis=1)
        for h in hs:
            prod = jnp.dot(
                hidden[pl.ds(4 * h * half, 4 * half), :hid], w, preferred_element_type=F32
            ).astype(BF16)
            for j, s in enumerate(slots):
                for e in range(4):
                    OP[s, e % 2, 2 * h + e // 2, :, c0:c0 + nc] = prod[e * half:(e + 1) * half, j * nc:(j + 1) * nc]
        for s in slots:
            start(remote(OP.at[s, 1 - t, two, :, cs], RO.at[s, two, :, cs], gone.at[10], o_r.at[sem], s_dev))

    def down_pair(k, *hs):
        slots, _ = groups[k]
        n, cs, two, rows, sem = span(k, hs)
        landed(RO.at[pl.ds(0, n), two, :, cs], o_r.at[sem])
        for s in slots:
            for h in hs:
                c = 2 * h + 1 - p
                ZC[s, h, :, cs] = (OP[s, t, c, :, cs].astype(F32) + RO[s, c, :, cs].astype(F32)).astype(BF16)
            start(remote(ZC.at[s, rows, :, cs], RF.at[s, rows, :, cs], gone.at[11], q_r.at[sem], z_dev))

    def finish(k, *hs):
        slots, (c0, nc) = groups[k]
        n, cs, _, rows, sem = span(k, hs)
        landed(RF.at[pl.ds(0, n), rows, :, cs], q_r.at[sem])
        for s in slots:
            for h in hs:
                c = 2 * h + p
                for a in range(0, nc, LANES):
                    lo = c0 + a
                    q, at = lo // mcols, lo % mcols
                    cs = pl.ds(lo, LANES)
                    ms = pl.ds(pl.multiple_of(s * mcols + at, LANES), LANES)
                    whole = pl.ds(pl.multiple_of(s * cols + lo, LANES), LANES)
                    stream = tok[part(c, t), whole].astype(F32) + BR[q, c, :, ms].astype(F32)
                    branch = (
                        OP[s, t, c, :, cs].astype(F32)
                        + RO[s, c, :, cs].astype(F32)
                        + RF[s, h, :, cs].astype(F32)
                    )
                    out[h * half:(h + 1) * half, whole] = (stream + branch).astype(BF16)

    def later(*cs):
        for c in cs:
            landed(n2.at[part(c, 1 - t)], n_r.at[c])

    if role:
        mix_in(0)
        mix_in(1)
        mix_in(2)
        step(4, 6)
        mix_in(3)
        arrived(2, 3)
        mix_out(0)
        mix_out(1)
        mix_pair(0)
        step(5, 7)
        mix_out(2)
        mix_pair(1)
        across(4)
        mix_out(3)
        mix_pair(2)
        mix_pair(3)
        step(6, 8)
        stream_chunk(0)
        across(5)
        stream_chunk(1)
        step(7)
        later(0, 1)
        arrived(4)
        ffn_rows(4, 0)
        across(6)
        arrived(5)
        ffn_rows(5, 0)
        stream_chunk(2)
        step(8, 9, 10, 11)
        across(7)
        stream_chunk(3)
        later(2, 3)
        ffn_rows(4, 1)
        ffn_rows(5, 1)
        across(8)
        arrived(6)
        ffn_rows(6, 0)
        ffn_rows(6, 1)
        arrived(7)
        ffn_rows(7, 0)
        arrived(8)
        ffn_rows(8, 0)
        down_send(0, 0)
        ffn_rows(7, 1)
        ffn_rows(8, 1)
        down_pair(0, 0)
        down_send(0, 1)
        step(9)
        sides(9)
        down_send(1, 0, 1)
        down_pair(0, 1)
        down_pair(1, 0, 1)
        step(10)
        finish(0, 0)
        step(11)
        sides(10)
        down_send(2, 0, 1)
        finish(0, 1)
        down_pair(2, 0, 1)
        sides(11)
        down_send(4, 0, 1)
        across(9)
        down_send(3, 0, 1)
        down_pair(4, 0, 1)
        across(10)
        down_pair(3, 0, 1)
        corner(10)
        down_send(5, 0, 1)
        across(11)
        down_pair(5, 0, 1)
        corner(11)
    else:
        mix_in(0)
        mix_in(1)
        step(2)
        mix_in(2)
        mix_in(3)
        step(3, 4, 5)
        arrived(2, 3)
        mix_out(0)
        mix_out(1)
        mix_pair(0)
        mix_out(2)
        mix_pair(1)
        step(4, 6)
        mix_out(3)
        mix_pair(2)
        mix_pair(3)
        stream_chunk(0)
        step(5, 7)
        stream_chunk(1)
        later(0, 1)
        arrived(4)
        ffn_rows(4, 0)
        step(6)
        stream_chunk(2)
        arrived(5)
        ffn_rows(5, 0)
        step(7, 8, 9)
        stream_chunk(3)
        later(2, 3)
        ffn_rows(4, 1)
        ffn_rows(5, 1)
        arrived(6)
        ffn_rows(6, 0)
        ffn_rows(6, 1)
        arrived(7)
        ffn_rows(7, 0)
        down_send(0, 0)
        ffn_rows(7, 1)
        down_pair(0, 0)
        down_send(0, 1)
        step(8, 10)
        down_pair(0, 1)
        step(9)
        down_send(1, 0, 1)
        down_pair(1, 0, 1)
        down_send(2, 0, 1)
        down_pair(2, 0, 1)
        across(8)
        step(10)
        down_send(4, 0, 1)
        down_send(3, 0, 1)
        down_pair(4, 0, 1)
        finish(0, 0)
        across(9)
        down_pair(3, 0, 1)
        down_send(5, 0, 1)
        finish(0, 1)
        across(10)
        down_pair(5, 0, 1)

    down_send(6, 0, 1)
    finish(1, 0, 1)
    down_pair(6, 0, 1)
    for k in (2, 4, 3, 5, 6):
        finish(k, 0, 1)
    for w, ref in enumerate((
        WA.at[pl.ds(0, 3)], WM.at[pl.ds(0, 3)], WG.at[pl.ds(0, 3), :, pl.ds(0, 2 * hid)],
        WD.at[pl.ds(0, 3), pl.ds(0, hid)], tok.at[pl.ds(0, 2 * half)], tok.at[pl.ds(0, 2 * half)],
        gated.at[role], RS, BR.at[role], n2.at[pl.ds(0, 4 * half)], RO, ZC,
    )):
        left(ref, w)


def paired_local(
    tokens, mix_gain, w_gate_b, w_gate_c, w_conv_in, conv_taps, w_mix_out, ffn_gain,
    w_ffn_gate, w_ffn_up, w_ffn_down,
):
    chip_rows, width = tokens.shape
    n_fs = lax.axis_size("fs")
    rows_d = w_gate_b.shape[0]
    ch = w_gate_b.shape[1] // 2
    units = inner_units(w_ffn_gate.shape[1])
    hid = units * LANES
    cols = w_mix_out.shape[1]
    half = chip_rows // 4
    group = 2 * chip_rows

    def vmem(*shape):
        return pltpu.VMEM(shape, BF16)

    def dma(*shape):
        return pltpu.SemaphoreType.DMA(shape)

    return pl.pallas_call(
        layer_kernel,
        out_shape=pltpu.VMEM((2 * half, width), BF16),
        in_specs=[pl.BlockSpec(memory_space=pl.ANY)] * 11,
        out_specs=pl.BlockSpec(memory_space=pltpu.VMEM),
        scratch_shapes=[
            vmem(group, width),
            vmem(group, width),
            vmem(group, width),
            vmem(n_fs, rows_d, 3 * ch),
            vmem(n_fs, 2 * ch, cols // 2),
            vmem(n_fs, rows_d, 2 * hid),
            vmem(n_fs, hid, cols),
            vmem(2, group, ch),
            vmem(group, width // 2),
            vmem(N_CHUNKS, half, width // 2),
            vmem(2, N_CHUNKS, half, width // 2),
            vmem(group, hid),
            vmem(n_fs, 2, N_CHUNKS, half, cols),
            vmem(n_fs, N_CHUNKS, half, cols),
            vmem(n_fs, 2, half, cols),
            vmem(n_fs, 2, half, cols),
            pltpu.VMEM((1, width), F32),
            pltpu.VMEM(conv_taps.shape, F32),
            pltpu.VMEM((1, width), F32),
            dma(11),
            dma(12),
            *[dma(N_PIECES)] * 4,
            *[dma(2)] * 2,
            *[dma(N_CHUNKS)] * 4,
            *[dma(14)] * 2,
        ],
        compiler_params=pltpu.CompilerParams(
            collective_id=0, has_side_effects=True, vmem_limit_bytes=60 * 2**20
        ),
    )(
        tokens, w_gate_b, w_gate_c, w_conv_in, w_mix_out, w_ffn_gate, w_ffn_up, w_ffn_down,
        mix_gain.reshape(1, width), conv_taps, ffn_gain.reshape(1, width),
    )


def causal_mix(product_in, conv_taps):
    shaped = product_in.reshape(product_in.shape[0] // LEN, LEN, product_in.shape[1])
    padded = jnp.pad(shaped, ((0, 0), (2, 0), (0, 0)))
    convolved = (
        conv_taps[0] * padded[:, :-2]
        + conv_taps[1] * padded[:, 1:-1]
        + conv_taps[2] * padded[:, 2:]
    )
    return convolved.reshape(product_in.shape)


def general_local(
    tokens, mix_gain, w_gate_b, w_gate_c, w_conv_in, conv_taps, w_mix_out, ffn_gain,
    w_ffn_gate, w_ffn_up, w_ffn_down,
):
    def scatter(product):
        return lax.psum_scatter(
            product.astype(BF16), "tp", scatter_dimension=0, tiled=True
        ).astype(F32)

    def dot(a, b):
        return jnp.dot(a, b, preferred_element_type=F32)

    def rows(w):
        return lax.all_gather(w, "fs", axis=0, tiled=True)

    normed = rms_scale(tokens.astype(F32), mix_gain).astype(BF16)
    gate_b, gate_c, conv_in = (dot(normed, rows(w)) for w in (w_gate_b, w_gate_c, w_conv_in))
    gated = (gate_b * causal_mix(gate_c * conv_in, conv_taps)).astype(BF16)
    row_count = normed.shape[0] // lax.axis_size("tp")
    branch = scatter(dot(gated, lax.all_gather(w_mix_out, "fs", axis=1, tiled=True)))
    own = lax.dynamic_slice_in_dim(tokens, lax.axis_index("tp") * row_count, row_count, 0)
    stream = own.astype(F32) + branch
    normed_two = lax.all_gather(
        rms_scale(stream, ffn_gain).astype(BF16), "tp", axis=0, tiled=True
    )
    hidden = (jax.nn.silu(dot(normed_two, rows(w_ffn_gate))) * dot(normed_two, rows(w_ffn_up))).astype(BF16)
    ffn_branch = scatter(dot(hidden, lax.all_gather(w_ffn_down, "fs", axis=1, tiled=True)))
    return (stream + ffn_branch).astype(BF16)


def solution(mesh):
    in_specs = (
        P(("rep", "fs"), None),
        P(),
        P("fs", "tp"),
        P("fs", "tp"),
        P("fs", "tp"),
        P(None, "tp"),
        P("tp", "fs"),
        P(),
        P("fs", "tp"),
        P("fs", "tp"),
        P("tp", "fs"),
    )
    out_specs = P(("rep", "fs", "tp"), None)
    size = mesh.shape
    square = size["tp"] == 2 and size["fs"] == 4 and size["rep"] == 4

    def local(*arrays):
        rows, width = arrays[0].shape
        channels, hidden = arrays[2].shape[1], arrays[8].shape[1]
        fits = (
            square
            and rows % (4 * LEN) == 0
            and channels % (2 * LANES) == 0
            and hidden % LANES == 0
            and hidden >= 11 * LANES
            and width % (16 * LANES) == 0
        )
        return (paired_local if fits else general_local)(*arrays)

    return jax.shard_map(local, mesh=mesh, in_specs=in_specs, out_specs=out_specs, check_vma=False)
```

```python
import jax
import jax.numpy as jnp
from jax import lax
from jax.experimental import pallas as pl
from jax.experimental.pallas import tpu as pltpu
from jax.sharding import PartitionSpec as P

LEN = 128
LANES = 128
EPSILON = 1e-06
MESH = pl.DeviceIdType.MESH
F32 = jnp.float32
BF16 = jnp.bfloat16


def rms_scale(values, gain):
    return values * lax.rsqrt(jnp.mean(values * values, axis=-1, keepdims=True) + EPSILON) * gain


N_CHUNKS = 4
TILE = 16


def inner_units(hidden):
    units = hidden // LANES
    return (7 * units + 5) // 11


def tiles(rows, share):
    return int(rows * share) // TILE * TILE


def head_rows(role, rows):
    if role:
        return [0, rows // 4, 5 * rows // 8, rows]
    return [0, rows // 2, rows]


def weight_pieces(role, rows_d, n_conv, mix_rows, n_mix, units, hid, n_down):
    starts = head_rows(role, rows_d)
    head = [(0, a, b - a, 0, n_conv, 0.375) for a, b in zip(starts, starts[1:])]
    pieces = head[:2]
    pieces += [(1, i * mix_rows // 2, mix_rows // 2, 0, n_mix, 0.375) for i in range(2)]
    cuts = [i * units // 4 for i in range(4)] + [units]
    if role:
        cuts = [(u * units + 6) // 7 for u in (0, 1, 3, 5, 6)] + [units]
    pieces += [
        (2, 0, rows_d, 2 * LANES * a, 2 * LANES * (b - a), share)
        for a, b, share in zip(cuts, cuts[1:], (0.32, 0.32, 0.32, 0.32, 0.32))
    ]
    down = (0, n_down // 4, n_down // 2, n_down)
    for a, b, share in zip(down, down[1:], (0.4, 0.4, 0)):
        pieces.append((3, 0, hid, a, b - a, share))
    return pieces + head[2:]


N_PIECES = 13


def layer_kernel(*refs):
    r = lax.axis_index("rep")
    p = lax.rem(r, 2)
    f = lax.axis_index("fs")
    barrier = pltpu.get_barrier_semaphore()
    x_of = f + 1 - 2 * lax.rem(f, 2)
    for dev in (
        {"fs": x_of}, {"fs": lax.rem(f + 2, 4)}, {"rep": r + 1 - 2 * p}, {"tp": 1 - lax.axis_index("tp")}
    ):
        pl.semaphore_signal(barrier, inc=1, device_id=dev, device_id_type=MESH)
    inner = jnp.logical_or(r == 1, r == 2)

    @pl.when(inner)
    def _():
        layer_body(1, barrier, *refs)

    @pl.when(jnp.logical_not(inner))
    def _():
        layer_body(0, barrier, *refs)


def layer_body(
    role, barrier,
    tokens, wb, wc, wi, wm_in, wg_in, wu_in, wd_in, mix_gain_in, taps_in, ffn_gain_in,
    out,
    tok, normed, n2, WA, WM, WG, WD, gated, MP, RS, BR, hidden, OP, RO, ZC, RF, mix_gain, taps, ffn_gain,
    load_sem, gone, dr, fr, ur, cr, tz_r, ts_r, g_r, sib_r, z_r, n_r, o_r, q_r,
):
    n_fs, rows_d, _ = WA.shape
    ch = gated.shape[2]
    width = tokens.shape[1]
    half = tokens.shape[0] // 4
    cols = WD.shape[2]
    mcols = WM.shape[2]
    all_units = wg_in.shape[1] // LANES
    units = inner_units(wg_in.shape[1])
    first = 0
    if not role:
        first, units = units, all_units - units
    hid = units * LANES

    r = lax.axis_index("rep")
    f = lax.axis_index("fs")
    t = lax.axis_index("tp")
    p = lax.rem(r, 2)
    twin = r - 1
    z_dev = {"rep": r + 1 - 2 * p}
    w_dev = {"rep": 3 - r}
    x_of = f + 1 - 2 * lax.rem(f, 2)
    y_of = lax.rem(f + 2, 4)
    d_of = lax.rem(x_of + 2, 4)
    x_dev, y_dev, s_dev = {"fs": x_of}, {"fs": y_of}, {"tp": 1 - t}

    def part(c, core):
        return pl.ds(pl.multiple_of((2 * c + core) * half, half), half)

    def chunk(c):
        return pl.ds(pl.multiple_of(2 * c * half, 2 * half), 2 * half)

    if role:
        pl.semaphore_signal(barrier, inc=1, device_id=w_dev, device_id_type=MESH)

    chan = pl.ds(role * ch, ch)
    def load(src, dst, k):
        pltpu.make_async_copy(src, dst, load_sem.at[k]).start()

    def loaded(ref, k):
        pltpu.make_async_copy(ref, ref, load_sem.at[k]).wait()

    starts = head_rows(role, rows_d)
    w_rows = [pl.ds(a, b - a) for a, b in zip(starts, starts[1:])]
    for k in range(len(w_rows)):
        for i, w in enumerate((wb, wc, wi)):
            load(w.at[w_rows[k], chan], WA.at[f, w_rows[k], pl.ds(i * ch, ch)], (0, 1, 10)[k])
    for h in range(2):
        for core in range(2):
            load(tokens.at[pl.ds((2 * core + h) * half, half)], tok.at[part(2 * h + p, core)], 2)
    small = ((mix_gain_in, mix_gain), (taps_in, taps), (ffn_gain_in, ffn_gain))
    for i, (src, dst) in enumerate(small):
        load(src, dst, 3 + i)
    pl.semaphore_wait(barrier, 4 + role)

    def remote(src, dst, s, rcv, dev):
        return pltpu.make_async_remote_copy(
            src_ref=src, dst_ref=dst, send_sem=s, recv_sem=rcv, device_id=dev, device_id_type=MESH
        )

    bufs = (WA, WM, WG, WD)
    pieces = weight_pieces(role, rows_d, 3 * ch, WM.shape[1], mcols, units, hid, cols)

    def cut(k, slot, lo, n):
        w, r0, _, c0, nc, _ = pieces[k]
        at = r0 + lo
        if not isinstance(at, int):
            at = pl.multiple_of(at, TILE)
        return bufs[w].at[slot, pl.ds(at, n), pl.ds(c0, nc)]

    def share(k):
        rows = pieces[k][2]
        lent = tiles(rows, pieces[k][5]) if role else 0
        kept = rows - lent
        near = tiles(kept, 0.5)
        lo = twin * lent if role else 0
        mine = twin * kept if role else 0
        return lent, kept, near, lo, mine

    def direct(k):
        _, kept, _, lo, _ = share(k)
        ref = cut(k, f, lo, kept)
        sem = gone.at[pieces[k][0]]
        return [remote(ref, ref, sem, dr.at[k], dev) for dev in (x_dev, y_dev)]

    def forward(k):
        _, kept, near, lo, _ = share(k)
        a, b = cut(k, x_of, lo, near), cut(k, y_of, lo + near, kept - near)
        return [
            remote(b, b, gone.at[pieces[k][0]], fr.at[k], x_dev),
            remote(a, a, gone.at[pieces[k][0]], fr.at[k], y_dev),
        ]

    def lend(k, sems, *slots):
        lent, _, _, _, mine = share(k)
        if not lent:
            return []
        refs = [cut(k, slot, mine, lent) for slot in slots]
        return [remote(ref, ref, gone.at[pieces[k][0]], sems.at[k], w_dev) for ref in refs]

    def start(*copies):
        for c in copies:
            c.start()

    def landed(ref, sem):
        remote(ref, ref, sem, sem, s_dev).wait_recv()

    def left(ref, k):
        remote(ref, ref, gone.at[k], gone.at[k], s_dev).wait_send()

    passed = set()

    def send(*ks):
        for k in ks:
            start(*direct(k))

    def step(k, *more):
        landed(cut(k, pl.ds(0, 2), 0, share(k)[1]), dr.at[k])
        start(*forward(k))
        if role:
            start(*lend(k, ur, x_of, y_of))
        send(*more)

    def across(*ks):
        for k in ks:
            if k not in passed:
                passed.add(k)
                landed(cut(k, 0, 0, share(k)[1]), fr.at[k])
                if role:
                    start(*lend(k, cr, d_of))

    def sides(*ks):
        for k in ks:
            if share(k)[0]:
                landed(cut(k, pl.ds(0, 2), 0, share(k)[0]), ur.at[k])

    def corner(*ks):
        across(*ks)
        for k in ks:
            if share(k)[0]:
                landed(cut(k, 0, 0, share(k)[0]), cr.at[k])

    def arrived(*ks):
        across(*ks)
        sides(*ks)
        corner(*ks)

    for k in range(len(w_rows)):
        loaded(WA.at[f, w_rows[k]], (0, 1, 10)[k])
        send((0, 1, 12)[k])
    loaded(tok.at[pl.ds(0, 4 * half)], 2)
    for i, (_, dst) in enumerate(small):
        loaded(dst, 3 + i)
    for h in range(2):
        ref = tok.at[part(2 * h + p, t)]
        start(remote(ref, ref, gone.at[4], tz_r.at[h], z_dev))

    def relay(h):
        ref = tok.at[part(2 * h + 1 - p, t)]
        landed(ref, tz_r.at[h])
        start(remote(ref, ref, gone.at[5], ts_r.at[h], s_dev))

    def sibling(h):
        landed(tok.at[part(2 * h, t)], ts_r.at[h])

    def norm_chunk(c):
        def body(i, _):
            rows = pl.ds(pl.multiple_of(2 * c * half + i * 64, 64), 64)
            normed[rows, :] = rms_scale(tok[rows, :].astype(F32), mix_gain[...]).astype(BF16)
            return 0

        lax.fori_loop(0, 2 * half // 64, body, 0)

    load(wm_in.at[:, pl.ds(role * mcols, mcols)], WM.at[f], 6)
    for c in range(units):
        for i, w in enumerate((wg_in, wu_in)):
            load(w.at[:, pl.ds((first + c) * LANES, LANES)], WG.at[f, :, pl.ds((2 * c + i) * LANES, LANES)], 7)
    load(wd_in.at[pl.ds(first * LANES, hid)], WD.at[f, pl.ds(0, hid)], 8)

    norm_chunk(p)
    norm_chunk(2 + p)
    loaded(WM.at[f], 6)
    loaded(WG.at[f, :, pl.ds(0, 2 * hid)], 7)
    loaded(WD.at[f, pl.ds(0, hid)], 8)
    step(0)
    if role:
        step(1)
    relay(0)
    if role:
        step(12, 2, 3)
        sibling(0)
        norm_chunk(1 - p)
        across(0)
        across(1)
        across(12)
        step(2)
        step(3, 4, 5)
        relay(1)
        sibling(1)
        norm_chunk(3 - p)
        across(2)
        across(3)
    else:
        sibling(0)
        norm_chunk(1 - p)
        step(1, 2, 3)
        relay(1)
        sibling(1)
        norm_chunk(3 - p)
    arrived(0, 1, *((12,) if role else ()))

    tap = [taps[pl.ds(i, 1), chan] for i in range(3)]
    pos = lax.rem(lax.broadcasted_iota(jnp.int32, (2 * half, ch), 0), LEN)

    def mix_in(c):
        x = normed[chunk(c), :]

        def proj(q):
            w = WA[:, :, q * ch:(q + 1) * ch].reshape(width, ch)
            return jnp.dot(x, w, preferred_element_type=F32)

        pr = proj(1) * proj(2)
        one = jnp.where(pos >= 1, pltpu.roll(pr, 1, 0), 0.0)
        two = jnp.where(pos >= 2, pltpu.roll(pr, 2, 0), 0.0)
        conv = tap[0] * two + tap[1] * one + tap[2] * pr
        gated[role, chunk(c), :] = (proj(0) * conv).astype(BF16)
        ref = gated.at[role, chunk(c)]
        start(remote(ref, ref, gone.at[6], g_r.at[c], z_dev))

    def mix_out(c):
        landed(gated.at[role, chunk(c)], g_r.at[c])
        g = jnp.concatenate([gated[0, chunk(c), :], gated[1, chunk(c), :]], axis=1)
        for s in range(n_fs):
            MP[chunk(c), s * mcols:(s + 1) * mcols] = jnp.dot(
                g, WM[s], preferred_element_type=F32
            ).astype(BF16)
        start(remote(MP.at[part(c, 1 - t)], RS.at[c], gone.at[7], sib_r.at[c], s_dev))

    def mix_pair(c):
        landed(RS.at[c], sib_r.at[c])
        BR[role, c] = (MP[part(c, t), :].astype(F32) + RS[c].astype(F32)).astype(BF16)
        start(remote(BR.at[role, c], BR.at[role, c], gone.at[8], z_r.at[c], z_dev))

    def stream_chunk(c):
        landed(BR.at[1 - role, c], z_r.at[c])
        step_rows = 32

        def body(i, _):
            rows = pl.ds(pl.multiple_of(i * step_rows, step_rows), step_rows)
            mine = pl.ds(pl.multiple_of((2 * c + t) * half + i * step_rows, step_rows), step_rows)
            branch = jnp.concatenate(
                [BR[q, c, rows, s * mcols:(s + 1) * mcols] for s in range(n_fs) for q in range(2)], axis=1
            )
            stream = tok[mine, :].astype(F32) + branch.astype(F32)
            n2[mine, :] = rms_scale(stream, ffn_gain[...]).astype(BF16)
            return 0

        lax.fori_loop(0, half // step_rows, body, 0)
        ref = n2.at[part(c, t)]
        start(remote(ref, ref, gone.at[9], n_r.at[c], s_dev))

    def ffn_rows(k, i):
        _, _, _, c0, nc, _ = pieces[k]
        cuts = 2 if nc == 2 * LANES else 1
        n = 4 * half // cuts
        for a in range(c0, c0 + nc, 2 * LANES):
            w = WG[:, :, a:a + 2 * LANES].reshape(width, 2 * LANES)
            for j in range(cuts):
                rows = pl.ds(4 * i * half + j * n, n)
                zz = jnp.dot(n2[rows, :], w, preferred_element_type=F32)
                g, u = zz[:, :LANES], zz[:, LANES:]
                hidden[rows, a // 2:a // 2 + LANES] = (g / (1.0 + jnp.exp(-g)) * u).astype(BF16)

    dn = (9, 10, 11) if role else (8, 9, 10)
    cuts = [pieces[k][3:5] for k in dn]
    groups = [
        ((f,), (0, cols)), ((x_of, y_of), cuts[0]), ((x_of, y_of), cuts[1]), ((d_of,), cuts[0]),
        ((x_of, y_of), cuts[2]), ((d_of,), cuts[1]), ((d_of,), cuts[2]),
    ]
    def span(k, hs):
        n = len(groups[k][0])
        return n, pl.ds(*groups[k][1]), pl.ds(2 * hs[0], 2 * len(hs)), pl.ds(hs[0], len(hs)), 7 * hs[0] + k

    def down_send(k, *hs):
        slots, (c0, nc) = groups[k]
        _, cs, two, _, sem = span(k, hs)
        w = jnp.concatenate([WD[s, :hid, c0:c0 + nc] for s in slots], axis=1)
        for h in hs:
            prod = jnp.dot(
                hidden[pl.ds(4 * h * half, 4 * half), :hid], w, preferred_element_type=F32
            ).astype(BF16)
            for j, s in enumerate(slots):
                for e in range(4):
                    OP[s, e % 2, 2 * h + e // 2, :, c0:c0 + nc] = prod[e * half:(e + 1) * half, j * nc:(j + 1) * nc]
        for s in slots:
            start(remote(OP.at[s, 1 - t, two, :, cs], RO.at[s, two, :, cs], gone.at[10], o_r.at[sem], s_dev))

    def down_pair(k, *hs):
        slots, _ = groups[k]
        n, cs, two, rows, sem = span(k, hs)
        landed(RO.at[pl.ds(0, n), two, :, cs], o_r.at[sem])
        for s in slots:
            for h in hs:
                c = 2 * h + 1 - p
                ZC[s, h, :, cs] = (OP[s, t, c, :, cs].astype(F32) + RO[s, c, :, cs].astype(F32)).astype(BF16)
            start(remote(ZC.at[s, rows, :, cs], RF.at[s, rows, :, cs], gone.at[11], q_r.at[sem], z_dev))

    def finish(k, *hs):
        slots, (c0, nc) = groups[k]
        n, cs, _, rows, sem = span(k, hs)
        landed(RF.at[pl.ds(0, n), rows, :, cs], q_r.at[sem])
        for s in slots:
            for h in hs:
                c = 2 * h + p
                for a in range(0, nc, LANES):
                    lo = c0 + a
                    q, at = lo // mcols, lo % mcols
                    cs = pl.ds(lo, LANES)
                    ms = pl.ds(pl.multiple_of(s * mcols + at, LANES), LANES)
                    whole = pl.ds(pl.multiple_of(s * cols + lo, LANES), LANES)
                    stream = tok[part(c, t), whole].astype(F32) + BR[q, c, :, ms].astype(F32)
                    branch = (
                        OP[s, t, c, :, cs].astype(F32)
                        + RO[s, c, :, cs].astype(F32)
                        + RF[s, h, :, cs].astype(F32)
                    )
                    out[h * half:(h + 1) * half, whole] = (stream + branch).astype(BF16)

    def later(*cs):
        for c in cs:
            landed(n2.at[part(c, 1 - t)], n_r.at[c])

    if role:
        mix_in(0)
        mix_in(1)
        mix_in(2)
        step(4, 6)
        mix_in(3)
        arrived(2, 3)
        mix_out(0)
        mix_out(1)
        mix_pair(0)
        step(5, 7)
        mix_out(2)
        mix_pair(1)
        across(4)
        mix_out(3)
        mix_pair(2)
        mix_pair(3)
        step(6, 8)
        stream_chunk(0)
        across(5)
        stream_chunk(1)
        step(7)
        later(0, 1)
        arrived(4)
        ffn_rows(4, 0)
        across(6)
        arrived(5)
        ffn_rows(5, 0)
        stream_chunk(2)
        step(8, 9, 10, 11)
        across(7)
        stream_chunk(3)
        later(2, 3)
        ffn_rows(4, 1)
        ffn_rows(5, 1)
        across(8)
        arrived(6)
        ffn_rows(6, 0)
        step(9)
        ffn_rows(6, 1)
        arrived(7)
        ffn_rows(7, 0)
        arrived(8)
        ffn_rows(8, 0)
        step(10)
        down_send(0, 0)
        ffn_rows(7, 1)
        ffn_rows(8, 1)
        down_pair(0, 0)
        down_send(0, 1)
        sides(9)
        down_send(1, 0, 1)
        down_pair(0, 1)
        down_pair(1, 0, 1)
        sides(10)
        down_send(2, 0, 1)
        step(11)
        down_pair(2, 0, 1)
        down_send(4, 0, 1)
        across(9)
        down_pair(4, 0, 1)
        across(10)
        finish(0, 0)
        finish(0, 1)
        corner(9)
        down_send(3, 0, 1)
        corner(10)
        down_send(5, 0, 1)
        down_pair(3, 0, 1)
        across(11)
        down_send(6, 0, 1)
        down_pair(5, 0, 1)
    else:
        mix_in(0)
        mix_in(1)
        step(2)
        mix_in(2)
        mix_in(3)
        step(3, 4, 5)
        arrived(2, 3)
        mix_out(0)
        mix_out(1)
        mix_pair(0)
        mix_out(2)
        mix_pair(1)
        step(4, 6)
        mix_out(3)
        mix_pair(2)
        mix_pair(3)
        stream_chunk(0)
        step(5, 7)
        stream_chunk(1)
        later(0, 1)
        arrived(4)
        ffn_rows(4, 0)
        step(6)
        stream_chunk(2)
        arrived(5)
        ffn_rows(5, 0)
        step(7, 8, 9)
        stream_chunk(3)
        later(2, 3)
        ffn_rows(4, 1)
        ffn_rows(5, 1)
        arrived(6)
        ffn_rows(6, 0)
        ffn_rows(6, 1)
        arrived(7)
        ffn_rows(7, 0)
        down_send(0, 0)
        ffn_rows(7, 1)
        down_pair(0, 0)
        down_send(0, 1)
        step(8, 10)
        down_pair(0, 1)
        step(9)
        down_send(1, 0, 1)
        down_send(2, 0, 1)
        down_pair(1, 0, 1)
        down_pair(2, 0, 1)
        finish(0, 0)
        step(10)
        down_send(4, 0, 1)
        across(8)
        across(9)
        down_send(3, 0, 1)
        down_send(5, 0, 1)
        down_pair(4, 0, 1)
        down_pair(3, 0, 1)
        down_pair(5, 0, 1)
        finish(0, 1)
        across(10)
        down_send(6, 0, 1)

    finish(1, 0, 1)
    down_pair(6, 0, 1)
    for k in (2, 4, 3, 5, 6):
        finish(k, 0, 1)
    for w, ref in enumerate((
        WA.at[pl.ds(0, 3)], WM.at[pl.ds(0, 3)], WG.at[pl.ds(0, 3), :, pl.ds(0, 2 * hid)],
        WD.at[pl.ds(0, 3), pl.ds(0, hid)], tok.at[pl.ds(0, 2 * half)], tok.at[pl.ds(0, 2 * half)],
        gated.at[role], RS, BR.at[role], n2.at[pl.ds(0, 4 * half)], RO, ZC,
    )):
        left(ref, w)


def paired_local(
    tokens, mix_gain, w_gate_b, w_gate_c, w_conv_in, conv_taps, w_mix_out, ffn_gain,
    w_ffn_gate, w_ffn_up, w_ffn_down,
):
    chip_rows, width = tokens.shape
    n_fs = lax.axis_size("fs")
    rows_d = w_gate_b.shape[0]
    ch = w_gate_b.shape[1] // 2
    units = inner_units(w_ffn_gate.shape[1])
    hid = units * LANES
    cols = w_mix_out.shape[1]
    half = chip_rows // 4
    group = 2 * chip_rows

    def vmem(*shape):
        return pltpu.VMEM(shape, BF16)

    def dma(*shape):
        return pltpu.SemaphoreType.DMA(shape)

    return pl.pallas_call(
        layer_kernel,
        out_shape=pltpu.VMEM((2 * half, width), BF16),
        in_specs=[pl.BlockSpec(memory_space=pl.ANY)] * 11,
        out_specs=pl.BlockSpec(memory_space=pltpu.VMEM),
        scratch_shapes=[
            vmem(group, width),
            vmem(group, width),
            vmem(group, width),
            vmem(n_fs, rows_d, 3 * ch),
            vmem(n_fs, 2 * ch, cols // 2),
            vmem(n_fs, rows_d, 2 * hid),
            vmem(n_fs, hid, cols),
            vmem(2, group, ch),
            vmem(group, width // 2),
            vmem(N_CHUNKS, half, width // 2),
            vmem(2, N_CHUNKS, half, width // 2),
            vmem(group, hid),
            vmem(n_fs, 2, N_CHUNKS, half, cols),
            vmem(n_fs, N_CHUNKS, half, cols),
            vmem(n_fs, 2, half, cols),
            vmem(n_fs, 2, half, cols),
            pltpu.VMEM((1, width), F32),
            pltpu.VMEM(conv_taps.shape, F32),
            pltpu.VMEM((1, width), F32),
            dma(11),
            dma(12),
            *[dma(N_PIECES)] * 4,
            *[dma(2)] * 2,
            *[dma(N_CHUNKS)] * 4,
            *[dma(14)] * 2,
        ],
        compiler_params=pltpu.CompilerParams(
            collective_id=0, has_side_effects=True, vmem_limit_bytes=60 * 2**20
        ),
    )(
        tokens, w_gate_b, w_gate_c, w_conv_in, w_mix_out, w_ffn_gate, w_ffn_up, w_ffn_down,
        mix_gain.reshape(1, width), conv_taps, ffn_gain.reshape(1, width),
    )


def causal_mix(product_in, conv_taps):
    shaped = product_in.reshape(product_in.shape[0] // LEN, LEN, product_in.shape[1])
    padded = jnp.pad(shaped, ((0, 0), (2, 0), (0, 0)))
    convolved = (
        conv_taps[0] * padded[:, :-2]
        + conv_taps[1] * padded[:, 1:-1]
        + conv_taps[2] * padded[:, 2:]
    )
    return convolved.reshape(product_in.shape)


def general_local(
    tokens, mix_gain, w_gate_b, w_gate_c, w_conv_in, conv_taps, w_mix_out, ffn_gain,
    w_ffn_gate, w_ffn_up, w_ffn_down,
):
    def scatter(product):
        return lax.psum_scatter(
            product.astype(BF16), "tp", scatter_dimension=0, tiled=True
        ).astype(F32)

    def dot(a, b):
        return jnp.dot(a, b, preferred_element_type=F32)

    def rows(w):
        return lax.all_gather(w, "fs", axis=0, tiled=True)

    normed = rms_scale(tokens.astype(F32), mix_gain).astype(BF16)
    gate_b, gate_c, conv_in = (dot(normed, rows(w)) for w in (w_gate_b, w_gate_c, w_conv_in))
    gated = (gate_b * causal_mix(gate_c * conv_in, conv_taps)).astype(BF16)
    row_count = normed.shape[0] // lax.axis_size("tp")
    branch = scatter(dot(gated, lax.all_gather(w_mix_out, "fs", axis=1, tiled=True)))
    own = lax.dynamic_slice_in_dim(tokens, lax.axis_index("tp") * row_count, row_count, 0)
    stream = own.astype(F32) + branch
    normed_two = lax.all_gather(
        rms_scale(stream, ffn_gain).astype(BF16), "tp", axis=0, tiled=True
    )
    hidden = (jax.nn.silu(dot(normed_two, rows(w_ffn_gate))) * dot(normed_two, rows(w_ffn_up))).astype(BF16)
    ffn_branch = scatter(dot(hidden, lax.all_gather(w_ffn_down, "fs", axis=1, tiled=True)))
    return (stream + ffn_branch).astype(BF16)


def solution(mesh):
    in_specs = (
        P(("rep", "fs"), None),
        P(),
        P("fs", "tp"),
        P("fs", "tp"),
        P("fs", "tp"),
        P(None, "tp"),
        P("tp", "fs"),
        P(),
        P("fs", "tp"),
        P("fs", "tp"),
        P("tp", "fs"),
    )
    out_specs = P(("rep", "fs", "tp"), None)
    size = mesh.shape
    square = size["tp"] == 2 and size["fs"] == 4 and size["rep"] == 4

    def local(*arrays):
        rows, width = arrays[0].shape
        channels, hidden = arrays[2].shape[1], arrays[8].shape[1]
        fits = (
            square
            and rows % (4 * LEN) == 0
            and channels % (2 * LANES) == 0
            and hidden % LANES == 0
            and hidden >= 11 * LANES
            and width % (16 * LANES) == 0
        )
        return (paired_local if fits else general_local)(*arrays)

    return jax.shard_map(local, mesh=mesh, in_specs=in_specs, out_specs=out_specs, check_vma=False)
```

```python
import jax
import jax.numpy as jnp
from jax import lax
from jax.experimental import pallas as pl
from jax.experimental.pallas import tpu as pltpu
from jax.sharding import PartitionSpec as P

LEN = 128
LANES = 128
EPSILON = 1e-06
MESH = pl.DeviceIdType.MESH
F32 = jnp.float32
BF16 = jnp.bfloat16


def rms_scale(values, gain):
    return values * lax.rsqrt(jnp.mean(values * values, axis=-1, keepdims=True) + EPSILON) * gain


N_CHUNKS = 4
TILE = 16


def inner_units(hidden):
    units = hidden // LANES
    return (7 * units + 5) // 11


def tiles(rows, share):
    return int(rows * share) // TILE * TILE


def head_rows(role, rows):
    if role:
        return [0, rows // 4, 5 * rows // 8, rows]
    return [0, rows // 2, rows]


def weight_pieces(role, rows_d, n_conv, mix_rows, n_mix, units, hid, n_down):
    starts = head_rows(role, rows_d)
    head = [(0, a, b - a, 0, n_conv, 0.375) for a, b in zip(starts, starts[1:])]
    pieces = head[:2]
    pieces += [(1, i * mix_rows // 2, mix_rows // 2, 0, n_mix, 0.375) for i in range(2)]
    cuts = [i * units // 4 for i in range(4)] + [units]
    if role:
        cuts = [(u * units + 6) // 7 for u in (0, 1, 3, 5, 6)] + [units]
    pieces += [
        (2, 0, rows_d, 2 * LANES * a, 2 * LANES * (b - a), share)
        for a, b, share in zip(cuts, cuts[1:], (0.32, 0.32, 0.32, 0.25, 0.25))
    ]
    down = (0, n_down // 4, n_down // 2, n_down)
    for a, b, share in zip(down, down[1:], (0.45, 0.45, 0)):
        pieces.append((3, 0, hid, a, b - a, share))
    return pieces + head[2:]


N_PIECES = 13


def layer_kernel(*refs):
    r = lax.axis_index("rep")
    p = lax.rem(r, 2)
    f = lax.axis_index("fs")
    barrier = pltpu.get_barrier_semaphore()
    x_of = f + 1 - 2 * lax.rem(f, 2)
    for dev in (
        {"fs": x_of}, {"fs": lax.rem(f + 2, 4)}, {"rep": r + 1 - 2 * p}, {"tp": 1 - lax.axis_index("tp")}
    ):
        pl.semaphore_signal(barrier, inc=1, device_id=dev, device_id_type=MESH)
    inner = jnp.logical_or(r == 1, r == 2)

    @pl.when(inner)
    def _():
        layer_body(1, barrier, *refs)

    @pl.when(jnp.logical_not(inner))
    def _():
        layer_body(0, barrier, *refs)


def layer_body(
    role, barrier,
    tokens, wb, wc, wi, wm_in, wg_in, wu_in, wd_in, mix_gain_in, taps_in, ffn_gain_in,
    out,
    tok, normed, n2, WA, WM, WG, WD, gated, MP, RS, BR, hidden, OP, RO, ZC, RF, mix_gain, taps, ffn_gain,
    load_sem, gone, dr, fr, ur, cr, tz_r, ts_r, g_r, sib_r, z_r, n_r, o_r, q_r,
):
    n_fs, rows_d, _ = WA.shape
    ch = gated.shape[2]
    width = tokens.shape[1]
    half = tokens.shape[0] // 4
    cols = WD.shape[2]
    mcols = WM.shape[2]
    all_units = wg_in.shape[1] // LANES
    units = inner_units(wg_in.shape[1])
    first = 0
    if not role:
        first, units = units, all_units - units
    hid = units * LANES

    r = lax.axis_index("rep")
    f = lax.axis_index("fs")
    t = lax.axis_index("tp")
    p = lax.rem(r, 2)
    twin = r - 1
    z_dev = {"rep": r + 1 - 2 * p}
    w_dev = {"rep": 3 - r}
    x_of = f + 1 - 2 * lax.rem(f, 2)
    y_of = lax.rem(f + 2, 4)
    d_of = lax.rem(x_of + 2, 4)
    x_dev, y_dev, s_dev = {"fs": x_of}, {"fs": y_of}, {"tp": 1 - t}

    def part(c, core):
        return pl.ds(pl.multiple_of((2 * c + core) * half, half), half)

    def chunk(c):
        return pl.ds(pl.multiple_of(2 * c * half, 2 * half), 2 * half)

    if role:
        pl.semaphore_signal(barrier, inc=1, device_id=w_dev, device_id_type=MESH)

    chan = pl.ds(role * ch, ch)
    def load(src, dst, k):
        pltpu.make_async_copy(src, dst, load_sem.at[k]).start()

    def loaded(ref, k):
        pltpu.make_async_copy(ref, ref, load_sem.at[k]).wait()

    starts = head_rows(role, rows_d)
    w_rows = [pl.ds(a, b - a) for a, b in zip(starts, starts[1:])]
    for k in range(len(w_rows)):
        for i, w in enumerate((wb, wc, wi)):
            load(w.at[w_rows[k], chan], WA.at[f, w_rows[k], pl.ds(i * ch, ch)], (0, 1, 9)[k])
    for h in range(2):
        for core in range(2):
            load(tokens.at[pl.ds((2 * core + h) * half, half)], tok.at[part(2 * h + p, core)], 2)
    small = ((mix_gain_in, mix_gain), (taps_in, taps), (ffn_gain_in, ffn_gain))
    for i, (src, dst) in enumerate(small):
        load(src, dst, 3 + i)
    pl.semaphore_wait(barrier, 4 + role)

    def remote(src, dst, s, rcv, dev):
        return pltpu.make_async_remote_copy(
            src_ref=src, dst_ref=dst, send_sem=s, recv_sem=rcv, device_id=dev, device_id_type=MESH
        )

    bufs = (WA, WM, WG, WD)
    pieces = weight_pieces(role, rows_d, 3 * ch, WM.shape[1], mcols, units, hid, cols)

    def cut(k, slot, lo, n):
        w, r0, _, c0, nc, _ = pieces[k]
        at = r0 + lo
        if not isinstance(at, int):
            at = pl.multiple_of(at, TILE)
        return bufs[w].at[slot, pl.ds(at, n), pl.ds(c0, nc)]

    def share(k):
        rows = pieces[k][2]
        lent = tiles(rows, pieces[k][5]) if role else 0
        kept = rows - lent
        near = tiles(kept, 0.5)
        lo = twin * lent if role else 0
        mine = twin * kept if role else 0
        return lent, kept, near, lo, mine

    def direct(k):
        _, kept, _, lo, _ = share(k)
        ref = cut(k, f, lo, kept)
        sem = gone.at[pieces[k][0]]
        return [remote(ref, ref, sem, dr.at[k], dev) for dev in (x_dev, y_dev)]

    def forward(k):
        _, kept, near, lo, _ = share(k)
        a, b = cut(k, x_of, lo, near), cut(k, y_of, lo + near, kept - near)
        return [
            remote(b, b, gone.at[pieces[k][0]], fr.at[k], x_dev),
            remote(a, a, gone.at[pieces[k][0]], fr.at[k], y_dev),
        ]

    def lend(k, sems, *slots):
        lent, _, _, _, mine = share(k)
        if not lent:
            return []
        refs = [cut(k, slot, mine, lent) for slot in slots]
        return [remote(ref, ref, gone.at[pieces[k][0]], sems.at[k], w_dev) for ref in refs]

    def start(*copies):
        for c in copies:
            c.start()

    def landed(ref, sem):
        remote(ref, ref, sem, sem, s_dev).wait_recv()

    def left(ref, k):
        remote(ref, ref, gone.at[k], gone.at[k], s_dev).wait_send()

    passed = set()

    def send(*ks):
        for k in ks:
            start(*direct(k))

    def step(k, *more):
        landed(cut(k, pl.ds(0, 2), 0, share(k)[1]), dr.at[k])
        start(*forward(k))
        if role:
            start(*lend(k, ur, x_of, y_of))
        send(*more)

    def across(*ks):
        for k in ks:
            if k not in passed:
                passed.add(k)
                landed(cut(k, 0, 0, share(k)[1]), fr.at[k])
                if role:
                    start(*lend(k, cr, d_of))

    def sides(*ks):
        for k in ks:
            if share(k)[0]:
                landed(cut(k, pl.ds(0, 2), 0, share(k)[0]), ur.at[k])

    def corner(*ks):
        across(*ks)
        for k in ks:
            if share(k)[0]:
                landed(cut(k, 0, 0, share(k)[0]), cr.at[k])

    def arrived(*ks):
        across(*ks)
        sides(*ks)
        corner(*ks)

    for k in range(len(w_rows)):
        loaded(WA.at[f, w_rows[k]], (0, 1, 9)[k])
        send((0, 1, 12)[k])
    loaded(tok.at[pl.ds(0, 4 * half)], 2)
    for i, (_, dst) in enumerate(small):
        loaded(dst, 3 + i)
    for h in range(2):
        ref = tok.at[part(2 * h + p, t)]
        start(remote(ref, ref, gone.at[4], tz_r.at[h], z_dev))

    def relay(h):
        ref = tok.at[part(2 * h + 1 - p, t)]
        landed(ref, tz_r.at[h])
        start(remote(ref, ref, gone.at[5], ts_r.at[h], s_dev))

    def sibling(h):
        landed(tok.at[part(2 * h, t)], ts_r.at[h])

    def norm_chunk(c):
        def body(i, _):
            rows = pl.ds(pl.multiple_of(2 * c * half + i * 64, 64), 64)
            normed[rows, :] = rms_scale(tok[rows, :].astype(F32), mix_gain[...]).astype(BF16)
            return 0

        lax.fori_loop(0, 2 * half // 64, body, 0)

    load(wm_in.at[:, pl.ds(role * mcols, mcols)], WM.at[f], 6)
    for c in range(units):
        for i, w in enumerate((wg_in, wu_in)):
            load(w.at[:, pl.ds((first + c) * LANES, LANES)], WG.at[f, :, pl.ds((2 * c + i) * LANES, LANES)], 7)
    load(wd_in.at[pl.ds(first * LANES, hid)], WD.at[f, pl.ds(0, hid)], 8)

    norm_chunk(p)
    norm_chunk(2 + p)
    loaded(WM.at[f], 6)
    loaded(WG.at[f, :, pl.ds(0, 2 * hid)], 7)
    loaded(WD.at[f, pl.ds(0, hid)], 8)
    step(0)
    if role:
        step(1)
    relay(0)
    if role:
        step(12, 2, 3)
        sibling(0)
        norm_chunk(1 - p)
        across(0)
        across(1)
        across(12)
        step(2)
        step(3, 4, 5)
        relay(1)
        sibling(1)
        norm_chunk(3 - p)
        across(2)
        across(3)
    else:
        sibling(0)
        norm_chunk(1 - p)
        step(1, 2, 3)
        relay(1)
        sibling(1)
        norm_chunk(3 - p)
    arrived(0, 1, *((12,) if role else ()))

    tap = [taps[pl.ds(i, 1), chan] for i in range(3)]
    pos = lax.rem(lax.broadcasted_iota(jnp.int32, (2 * half, ch), 0), LEN)

    def mix_in(c):
        x = normed[chunk(c), :]

        def proj(q):
            w = WA[:, :, q * ch:(q + 1) * ch].reshape(width, ch)
            return jnp.dot(x, w, preferred_element_type=F32)

        pr = proj(1) * proj(2)
        one = jnp.where(pos >= 1, pltpu.roll(pr, 1, 0), 0.0)
        two = jnp.where(pos >= 2, pltpu.roll(pr, 2, 0), 0.0)
        conv = tap[0] * two + tap[1] * one + tap[2] * pr
        gated[role, chunk(c), :] = (proj(0) * conv).astype(BF16)
        ref = gated.at[role, chunk(c)]
        start(remote(ref, ref, gone.at[6], g_r.at[c], z_dev))

    def mix_out(c):
        landed(gated.at[role, chunk(c)], g_r.at[c])
        g = jnp.concatenate([gated[0, chunk(c), :], gated[1, chunk(c), :]], axis=1)
        for s in range(n_fs):
            MP[chunk(c), s * mcols:(s + 1) * mcols] = jnp.dot(
                g, WM[s], preferred_element_type=F32
            ).astype(BF16)
        start(remote(MP.at[part(c, 1 - t)], RS.at[c], gone.at[7], sib_r.at[c], s_dev))

    def mix_pair(c):
        landed(RS.at[c], sib_r.at[c])
        BR[role, c] = (MP[part(c, t), :].astype(F32) + RS[c].astype(F32)).astype(BF16)
        start(remote(BR.at[role, c], BR.at[role, c], gone.at[8], z_r.at[c], z_dev))

    def stream_chunk(c):
        landed(BR.at[1 - role, c], z_r.at[c])
        step_rows = 32

        def body(i, _):
            rows = pl.ds(pl.multiple_of(i * step_rows, step_rows), step_rows)
            mine = pl.ds(pl.multiple_of((2 * c + t) * half + i * step_rows, step_rows), step_rows)
            branch = jnp.concatenate(
                [BR[q, c, rows, s * mcols:(s + 1) * mcols] for s in range(n_fs) for q in range(2)], axis=1
            )
            stream = tok[mine, :].astype(F32) + branch.astype(F32)
            n2[mine, :] = rms_scale(stream, ffn_gain[...]).astype(BF16)
            return 0

        lax.fori_loop(0, half // step_rows, body, 0)
        ref = n2.at[part(c, t)]
        start(remote(ref, ref, gone.at[9], n_r.at[c], s_dev))

    def ffn_rows(k, i):
        _, _, _, c0, nc, _ = pieces[k]
        cuts = 2 if nc == 2 * LANES else 1
        n = 4 * half // cuts
        for a in range(c0, c0 + nc, 2 * LANES):
            w = WG[:, :, a:a + 2 * LANES].reshape(width, 2 * LANES)
            for j in range(cuts):
                rows = pl.ds(4 * i * half + j * n, n)
                zz = jnp.dot(n2[rows, :], w, preferred_element_type=F32)
                g, u = zz[:, :LANES], zz[:, LANES:]
                hidden[rows, a // 2:a // 2 + LANES] = (g / (1.0 + jnp.exp(-g)) * u).astype(BF16)

    dn = (9, 10, 11) if role else (8, 9, 10)
    cuts = [pieces[k][3:5] for k in dn]
    groups = [
        ((f,), (0, cols)), ((x_of, y_of), cuts[0]), ((x_of, y_of), cuts[1]), ((d_of,), cuts[0]),
        ((x_of, y_of), cuts[2]), ((d_of,), cuts[1]), ((d_of,), cuts[2]),
    ]
    def span(k, hs):
        n = len(groups[k][0])
        return n, pl.ds(*groups[k][1]), pl.ds(2 * hs[0], 2 * len(hs)), pl.ds(hs[0], len(hs)), 7 * hs[0] + k

    def down_send(k, *hs):
        slots, (c0, nc) = groups[k]
        _, cs, two, _, sem = span(k, hs)
        w = jnp.concatenate([WD[s, :hid, c0:c0 + nc] for s in slots], axis=1)
        for h in hs:
            prod = jnp.dot(
                hidden[pl.ds(4 * h * half, 4 * half), :hid], w, preferred_element_type=F32
            ).astype(BF16)
            for j, s in enumerate(slots):
                for e in range(4):
                    OP[s, e % 2, 2 * h + e // 2, :, c0:c0 + nc] = prod[e * half:(e + 1) * half, j * nc:(j + 1) * nc]
        for s in slots:
            start(remote(OP.at[s, 1 - t, two, :, cs], RO.at[s, two, :, cs], gone.at[10], o_r.at[sem], s_dev))

    def down_pair(k, *hs):
        slots, _ = groups[k]
        n, cs, two, rows, sem = span(k, hs)
        landed(RO.at[pl.ds(0, n), two, :, cs], o_r.at[sem])
        for s in slots:
            for h in hs:
                c = 2 * h + 1 - p
                ZC[s, h, :, cs] = (OP[s, t, c, :, cs].astype(F32) + RO[s, c, :, cs].astype(F32)).astype(BF16)
            start(remote(ZC.at[s, rows, :, cs], RF.at[s, rows, :, cs], gone.at[11], q_r.at[sem], z_dev))

    def finish(k, *hs):
        slots, (c0, nc) = groups[k]
        n, cs, _, rows, sem = span(k, hs)
        landed(RF.at[pl.ds(0, n), rows, :, cs], q_r.at[sem])
        for s in slots:
            for h in hs:
                c = 2 * h + p
                for a in range(0, nc, LANES):
                    lo = c0 + a
                    q, at = lo // mcols, lo % mcols
                    cs = pl.ds(lo, LANES)
                    ms = pl.ds(pl.multiple_of(s * mcols + at, LANES), LANES)
                    whole = pl.ds(pl.multiple_of(s * cols + lo, LANES), LANES)
                    stream = tok[part(c, t), whole].astype(F32) + BR[q, c, :, ms].astype(F32)
                    branch = (
                        OP[s, t, c, :, cs].astype(F32)
                        + RO[s, c, :, cs].astype(F32)
                        + RF[s, h, :, cs].astype(F32)
                    )
                    out[h * half:(h + 1) * half, whole] = (stream + branch).astype(BF16)

    def later(*cs):
        for c in cs:
            landed(n2.at[part(c, 1 - t)], n_r.at[c])

    if role:
        mix_in(0)
        mix_in(1)
        mix_in(2)
        step(4, 6)
        mix_in(3)
        arrived(2, 3)
        mix_out(0)
        mix_out(1)
        mix_pair(0)
        step(5, 7)
        mix_out(2)
        mix_pair(1)
        across(4)
        mix_out(3)
        mix_pair(2)
        mix_pair(3)
        step(6, 8)
        stream_chunk(0)
        across(5)
        stream_chunk(1)
        step(7)
        later(0, 1)
        arrived(4)
        ffn_rows(4, 0)
        across(6)
        arrived(5)
        ffn_rows(5, 0)
        stream_chunk(2)
        step(8, 9, 10, 11)
        stream_chunk(3)
        across(7)
        later(2, 3)
        ffn_rows(4, 1)
        across(8)
        ffn_rows(5, 1)
        arrived(6)
        ffn_rows(6, 0)
        step(9)
        arrived(7)
        ffn_rows(7, 0)
        arrived(8)
        ffn_rows(8, 0)
        down_send(0, 0)
        step(10)
        ffn_rows(6, 1)
        down_pair(0, 0)
        ffn_rows(7, 1)
        ffn_rows(8, 1)
        down_send(0, 1)
        sides(9)
        down_send(1, 0, 1)
        down_pair(0, 1)
        down_pair(1, 0, 1)
        sides(10)
        down_send(2, 0, 1)
        step(11)
        down_pair(2, 0, 1)
        down_send(4, 0, 1)
        across(9)
        down_pair(4, 0, 1)
        across(10)
        finish(0, 0)
        finish(0, 1)
        corner(9)
        down_send(3, 0, 1)
        corner(10)
        down_send(5, 0, 1)
        down_pair(3, 0, 1)
        across(11)
        down_send(6, 0, 1)
        down_pair(5, 0, 1)
    else:
        mix_in(0)
        mix_in(1)
        step(2)
        mix_in(2)
        mix_in(3)
        step(3, 4, 5)
        arrived(2, 3)
        mix_out(0)
        mix_out(1)
        mix_pair(0)
        mix_out(2)
        mix_pair(1)
        step(4, 6)
        mix_out(3)
        mix_pair(2)
        mix_pair(3)
        stream_chunk(0)
        step(5, 7)
        stream_chunk(1)
        later(0, 1)
        arrived(4)
        ffn_rows(4, 0)
        step(6)
        stream_chunk(2)
        arrived(5)
        ffn_rows(5, 0)
        step(7, 8, 9)
        stream_chunk(3)
        later(2, 3)
        ffn_rows(4, 1)
        ffn_rows(5, 1)
        arrived(6)
        ffn_rows(6, 0)
        ffn_rows(6, 1)
        arrived(7)
        ffn_rows(7, 0)
        down_send(0, 0)
        ffn_rows(7, 1)
        down_pair(0, 0)
        down_send(0, 1)
        step(8, 10)
        down_pair(0, 1)
        step(9)
        down_send(1, 0, 1)
        down_send(2, 0, 1)
        down_pair(1, 0, 1)
        down_pair(2, 0, 1)
        finish(0, 0)
        step(10)
        down_send(4, 0, 1)
        across(8)
        across(9)
        down_send(3, 0, 1)
        down_send(5, 0, 1)
        down_pair(4, 0, 1)
        down_pair(3, 0, 1)
        down_pair(5, 0, 1)
        finish(0, 1)
        across(10)
        down_send(6, 0, 1)

    finish(1, 0, 1)
    down_pair(6, 0, 1)
    for k in (2, 4, 3, 5, 6):
        finish(k, 0, 1)
    for w, ref in enumerate((
        WA.at[pl.ds(0, 3)], WM.at[pl.ds(0, 3)], WG.at[pl.ds(0, 3), :, pl.ds(0, 2 * hid)],
        WD.at[pl.ds(0, 3), pl.ds(0, hid)], tok.at[pl.ds(0, 2 * half)], tok.at[pl.ds(0, 2 * half)],
        gated.at[role], RS, BR.at[role], n2.at[pl.ds(0, 4 * half)], RO, ZC,
    )):
        left(ref, w)


def paired_local(
    tokens, mix_gain, w_gate_b, w_gate_c, w_conv_in, conv_taps, w_mix_out, ffn_gain,
    w_ffn_gate, w_ffn_up, w_ffn_down,
):
    chip_rows, width = tokens.shape
    n_fs = lax.axis_size("fs")
    rows_d = w_gate_b.shape[0]
    ch = w_gate_b.shape[1] // 2
    units = inner_units(w_ffn_gate.shape[1])
    hid = units * LANES
    cols = w_mix_out.shape[1]
    half = chip_rows // 4
    group = 2 * chip_rows

    def vmem(*shape):
        return pltpu.VMEM(shape, BF16)

    def dma(*shape):
        return pltpu.SemaphoreType.DMA(shape)

    return pl.pallas_call(
        layer_kernel,
        out_shape=pltpu.VMEM((2 * half, width), BF16),
        in_specs=[pl.BlockSpec(memory_space=pl.ANY)] * 11,
        out_specs=pl.BlockSpec(memory_space=pltpu.VMEM),
        scratch_shapes=[
            vmem(group, width),
            vmem(group, width),
            vmem(group, width),
            vmem(n_fs, rows_d, 3 * ch),
            vmem(n_fs, 2 * ch, cols // 2),
            vmem(n_fs, rows_d, 2 * hid),
            vmem(n_fs, hid, cols),
            vmem(2, group, ch),
            vmem(group, width // 2),
            vmem(N_CHUNKS, half, width // 2),
            vmem(2, N_CHUNKS, half, width // 2),
            vmem(group, hid),
            vmem(n_fs, 2, N_CHUNKS, half, cols),
            vmem(n_fs, N_CHUNKS, half, cols),
            vmem(n_fs, 2, half, cols),
            vmem(n_fs, 2, half, cols),
            pltpu.VMEM((1, width), F32),
            pltpu.VMEM(conv_taps.shape, F32),
            pltpu.VMEM((1, width), F32),
            dma(10),
            dma(12),
            *[dma(N_PIECES)] * 4,
            *[dma(2)] * 2,
            *[dma(N_CHUNKS)] * 4,
            *[dma(8)] * 2,
        ],
        compiler_params=pltpu.CompilerParams(
            collective_id=0, has_side_effects=True, vmem_limit_bytes=60 * 2**20
        ),
    )(
        tokens, w_gate_b, w_gate_c, w_conv_in, w_mix_out, w_ffn_gate, w_ffn_up, w_ffn_down,
        mix_gain.reshape(1, width), conv_taps, ffn_gain.reshape(1, width),
    )


def causal_mix(product_in, conv_taps):
    shaped = product_in.reshape(product_in.shape[0] // LEN, LEN, product_in.shape[1])
    padded = jnp.pad(shaped, ((0, 0), (2, 0), (0, 0)))
    convolved = (
        conv_taps[0] * padded[:, :-2]
        + conv_taps[1] * padded[:, 1:-1]
        + conv_taps[2] * padded[:, 2:]
    )
    return convolved.reshape(product_in.shape)


def general_local(
    tokens, mix_gain, w_gate_b, w_gate_c, w_conv_in, conv_taps, w_mix_out, ffn_gain,
    w_ffn_gate, w_ffn_up, w_ffn_down,
):
    def scatter(product):
        return lax.psum_scatter(
            product.astype(BF16), "tp", scatter_dimension=0, tiled=True
        ).astype(F32)

    def dot(a, b):
        return jnp.dot(a, b, preferred_element_type=F32)

    def rows(w):
        return lax.all_gather(w, "fs", axis=0, tiled=True)

    normed = rms_scale(tokens.astype(F32), mix_gain).astype(BF16)
    gate_b, gate_c, conv_in = (dot(normed, rows(w)) for w in (w_gate_b, w_gate_c, w_conv_in))
    gated = (gate_b * causal_mix(gate_c * conv_in, conv_taps)).astype(BF16)
    row_count = normed.shape[0] // lax.axis_size("tp")
    branch = scatter(dot(gated, lax.all_gather(w_mix_out, "fs", axis=1, tiled=True)))
    own = lax.dynamic_slice_in_dim(tokens, lax.axis_index("tp") * row_count, row_count, 0)
    stream = own.astype(F32) + branch
    normed_two = lax.all_gather(
        rms_scale(stream, ffn_gain).astype(BF16), "tp", axis=0, tiled=True
    )
    hidden = (jax.nn.silu(dot(normed_two, rows(w_ffn_gate))) * dot(normed_two, rows(w_ffn_up))).astype(BF16)
    ffn_branch = scatter(dot(hidden, lax.all_gather(w_ffn_down, "fs", axis=1, tiled=True)))
    return (stream + ffn_branch).astype(BF16)


def solution(mesh):
    in_specs = (
        P(("rep", "fs"), None),
        P(),
        P("fs", "tp"),
        P("fs", "tp"),
        P("fs", "tp"),
        P(None, "tp"),
        P("tp", "fs"),
        P(),
        P("fs", "tp"),
        P("fs", "tp"),
        P("tp", "fs"),
    )
    out_specs = P(("rep", "fs", "tp"), None)
    size = mesh.shape
    square = size["tp"] == 2 and size["fs"] == 4 and size["rep"] == 4

    def local(*arrays):
        rows, width = arrays[0].shape
        channels, hidden = arrays[2].shape[1], arrays[8].shape[1]
        fits = (
            square
            and rows % (4 * LEN) == 0
            and channels % (2 * LANES) == 0
            and hidden % LANES == 0
            and hidden >= 11 * LANES
            and width % (16 * LANES) == 0
        )
        return (paired_local if fits else general_local)(*arrays)

    return jax.shard_map(local, mesh=mesh, in_specs=in_specs, out_specs=out_specs, check_vma=False)
```

```python
import jax
import jax.numpy as jnp
from jax import lax
from jax.experimental import pallas as pl
from jax.experimental.pallas import tpu as pltpu
from jax.sharding import PartitionSpec as P

LEN = 128
LANES = 128
EPSILON = 1e-06
MESH = pl.DeviceIdType.MESH
F32 = jnp.float32
BF16 = jnp.bfloat16


def rms_scale(values, gain):
    return values * lax.rsqrt(jnp.mean(values * values, axis=-1, keepdims=True) + EPSILON) * gain


N_CHUNKS = 4
TILE = 16


def inner_units(hidden):
    units = hidden // LANES
    return (7 * units + 5) // 11


def tiles(rows, share):
    return int(rows * share) // TILE * TILE


def head_rows(role, rows):
    if role:
        return [0, rows // 4, 5 * rows // 8, rows]
    return [0, rows // 2, rows]


def weight_pieces(role, rows_d, n_conv, mix_rows, n_mix, units, hid, n_down):
    starts = head_rows(role, rows_d)
    head = [(0, a, b - a, 0, n_conv, 0.42) for a, b in zip(starts, starts[1:])]
    pieces = head[:2]
    pieces += [(1, i * mix_rows // 2, mix_rows // 2, 0, n_mix, 0.375) for i in range(2)]
    cuts = [i * units // 4 for i in range(4)] + [units]
    if role:
        cuts = [(u * units + 6) // 7 for u in (0, 1, 3, 5, 6)] + [units]
    pieces += [
        (2, 0, rows_d, 2 * LANES * a, 2 * LANES * (b - a), share)
        for a, b, share in zip(cuts, cuts[1:], (0.32, 0.32, 0.32, 0.25, 0.25))
    ]
    down = (0, n_down // 4, n_down // 2, n_down)
    for a, b, share in zip(down, down[1:], (0.45, 0.45, 0)):
        pieces.append((3, 0, hid, a, b - a, share))
    return pieces + head[2:]


N_PIECES = 13


def layer_kernel(*refs):
    r = lax.axis_index("rep")
    p = lax.rem(r, 2)
    f = lax.axis_index("fs")
    barrier = pltpu.get_barrier_semaphore()
    x_of = f + 1 - 2 * lax.rem(f, 2)
    for dev in (
        {"fs": x_of}, {"fs": lax.rem(f + 2, 4)}, {"rep": r + 1 - 2 * p}, {"tp": 1 - lax.axis_index("tp")}
    ):
        pl.semaphore_signal(barrier, inc=1, device_id=dev, device_id_type=MESH)
    inner = jnp.logical_or(r == 1, r == 2)

    @pl.when(inner)
    def _():
        layer_body(1, barrier, *refs)

    @pl.when(jnp.logical_not(inner))
    def _():
        layer_body(0, barrier, *refs)


def layer_body(
    role, barrier,
    tokens, wb, wc, wi, wm_in, wg_in, wu_in, wd_in, mix_gain_in, taps_in, ffn_gain_in,
    out,
    tok, normed, n2, WA, WM, WG, WD, gated, MP, RS, BR, hidden, OP, RO, ZC, RF, mix_gain, taps, ffn_gain,
    load_sem, gone, dr, fr, ur, cr, tz_r, ts_r, g_r, sib_r, z_r, n_r, o_r, q_r,
):
    n_fs, rows_d, _ = WA.shape
    ch = gated.shape[2]
    width = tokens.shape[1]
    half = tokens.shape[0] // 4
    cols = WD.shape[2]
    mcols = WM.shape[2]
    all_units = wg_in.shape[1] // LANES
    units = inner_units(wg_in.shape[1])
    first = 0
    if not role:
        first, units = units, all_units - units
    hid = units * LANES

    r = lax.axis_index("rep")
    f = lax.axis_index("fs")
    t = lax.axis_index("tp")
    p = lax.rem(r, 2)
    twin = r - 1
    z_dev = {"rep": r + 1 - 2 * p}
    w_dev = {"rep": 3 - r}
    x_of = f + 1 - 2 * lax.rem(f, 2)
    y_of = lax.rem(f + 2, 4)
    d_of = lax.rem(x_of + 2, 4)
    x_dev, y_dev, s_dev = {"fs": x_of}, {"fs": y_of}, {"tp": 1 - t}

    def part(c, core):
        return pl.ds(pl.multiple_of((2 * c + core) * half, half), half)

    def chunk(c):
        return pl.ds(pl.multiple_of(2 * c * half, 2 * half), 2 * half)

    if role:
        pl.semaphore_signal(barrier, inc=1, device_id=w_dev, device_id_type=MESH)

    chan = pl.ds(role * ch, ch)
    def load(src, dst, k):
        pltpu.make_async_copy(src, dst, load_sem.at[k]).start()

    def loaded(ref, k):
        pltpu.make_async_copy(ref, ref, load_sem.at[k]).wait()

    starts = head_rows(role, rows_d)
    w_rows = [pl.ds(a, b - a) for a, b in zip(starts, starts[1:])]
    for k in range(len(w_rows)):
        for i, w in enumerate((wb, wc, wi)):
            load(w.at[w_rows[k], chan], WA.at[f, w_rows[k], pl.ds(i * ch, ch)], (0, 1, 9)[k])
    for h in range(2):
        for core in range(2):
            load(tokens.at[pl.ds((2 * core + h) * half, half)], tok.at[part(2 * h + p, core)], 2)
    small = ((mix_gain_in, mix_gain), (taps_in, taps), (ffn_gain_in, ffn_gain))
    for i, (src, dst) in enumerate(small):
        load(src, dst, 3 + i)
    pl.semaphore_wait(barrier, 4 + role)

    def remote(src, dst, s, rcv, dev):
        return pltpu.make_async_remote_copy(
            src_ref=src, dst_ref=dst, send_sem=s, recv_sem=rcv, device_id=dev, device_id_type=MESH
        )

    bufs = (WA, WM, WG, WD)
    pieces = weight_pieces(role, rows_d, 3 * ch, WM.shape[1], mcols, units, hid, cols)

    def cut(k, slot, lo, n):
        w, r0, _, c0, nc, _ = pieces[k]
        at = r0 + lo
        if not isinstance(at, int):
            at = pl.multiple_of(at, TILE)
        return bufs[w].at[slot, pl.ds(at, n), pl.ds(c0, nc)]

    def share(k):
        rows = pieces[k][2]
        lent = tiles(rows, pieces[k][5]) if role else 0
        kept = rows - lent
        near = tiles(kept, 0.5)
        lo = twin * lent if role else 0
        mine = twin * kept if role else 0
        return lent, kept, near, lo, mine

    def direct(k):
        _, kept, _, lo, _ = share(k)
        ref = cut(k, f, lo, kept)
        sem = gone.at[pieces[k][0]]
        return [remote(ref, ref, sem, dr.at[k], dev) for dev in (x_dev, y_dev)]

    def forward(k):
        _, kept, near, lo, _ = share(k)
        a, b = cut(k, x_of, lo, near), cut(k, y_of, lo + near, kept - near)
        return [
            remote(b, b, gone.at[pieces[k][0]], fr.at[k], x_dev),
            remote(a, a, gone.at[pieces[k][0]], fr.at[k], y_dev),
        ]

    def lend(k, sems, *slots):
        lent, _, _, _, mine = share(k)
        if not lent:
            return []
        refs = [cut(k, slot, mine, lent) for slot in slots]
        return [remote(ref, ref, gone.at[pieces[k][0]], sems.at[k], w_dev) for ref in refs]

    def start(*copies):
        for c in copies:
            c.start()

    def landed(ref, sem):
        remote(ref, ref, sem, sem, s_dev).wait_recv()

    def left(ref, k):
        remote(ref, ref, gone.at[k], gone.at[k], s_dev).wait_send()

    passed = set()

    def send(*ks):
        for k in ks:
            start(*direct(k))

    def step(k, *more):
        landed(cut(k, pl.ds(0, 2), 0, share(k)[1]), dr.at[k])
        start(*forward(k))
        if role:
            start(*lend(k, ur, x_of, y_of))
        send(*more)

    def across(*ks):
        for k in ks:
            if k not in passed:
                passed.add(k)
                landed(cut(k, 0, 0, share(k)[1]), fr.at[k])
                if role:
                    start(*lend(k, cr, d_of))

    def sides(*ks):
        for k in ks:
            if share(k)[0]:
                landed(cut(k, pl.ds(0, 2), 0, share(k)[0]), ur.at[k])

    def corner(*ks):
        across(*ks)
        for k in ks:
            if share(k)[0]:
                landed(cut(k, 0, 0, share(k)[0]), cr.at[k])

    def arrived(*ks):
        across(*ks)
        sides(*ks)
        corner(*ks)

    for k in range(len(w_rows)):
        loaded(WA.at[f, w_rows[k]], (0, 1, 9)[k])
        send((0, 1, 12)[k])
    loaded(tok.at[pl.ds(0, 4 * half)], 2)
    for i, (_, dst) in enumerate(small):
        loaded(dst, 3 + i)
    for h in range(2):
        ref = tok.at[part(2 * h + p, t)]
        start(remote(ref, ref, gone.at[4], tz_r.at[h], z_dev))

    def relay(h):
        ref = tok.at[part(2 * h + 1 - p, t)]
        landed(ref, tz_r.at[h])
        start(remote(ref, ref, gone.at[5], ts_r.at[h], s_dev))

    def sibling(h):
        landed(tok.at[part(2 * h, t)], ts_r.at[h])

    def norm_chunk(c):
        def body(i, _):
            rows = pl.ds(pl.multiple_of(2 * c * half + i * 64, 64), 64)
            normed[rows, :] = rms_scale(tok[rows, :].astype(F32), mix_gain[...]).astype(BF16)
            return 0

        lax.fori_loop(0, 2 * half // 64, body, 0)

    load(wm_in.at[:, pl.ds(role * mcols, mcols)], WM.at[f], 6)
    for c in range(units):
        for i, w in enumerate((wg_in, wu_in)):
            load(w.at[:, pl.ds((first + c) * LANES, LANES)], WG.at[f, :, pl.ds((2 * c + i) * LANES, LANES)], 7)
    load(wd_in.at[pl.ds(first * LANES, hid)], WD.at[f, pl.ds(0, hid)], 8)

    norm_chunk(p)
    norm_chunk(2 + p)
    loaded(WM.at[f], 6)
    loaded(WG.at[f, :, pl.ds(0, 2 * hid)], 7)
    loaded(WD.at[f, pl.ds(0, hid)], 8)
    step(0)
    if role:
        step(1)
    relay(0)
    if role:
        step(12, 2, 3)
        sibling(0)
        norm_chunk(1 - p)
        across(0)
        across(1)
        across(12)
        step(2)
        step(3, 4, 5)
        relay(1)
        sibling(1)
        norm_chunk(3 - p)
        across(2)
        across(3)
    else:
        sibling(0)
        norm_chunk(1 - p)
        step(1, 2, 3)
        relay(1)
        sibling(1)
        norm_chunk(3 - p)
    arrived(0, 1, *((12,) if role else ()))

    tap = [taps[pl.ds(i, 1), chan] for i in range(3)]
    pos = lax.rem(lax.broadcasted_iota(jnp.int32, (2 * half, ch), 0), LEN)

    def mix_in(c):
        x = normed[chunk(c), :]

        def proj(q):
            w = WA[:, :, q * ch:(q + 1) * ch].reshape(width, ch)
            return jnp.dot(x, w, preferred_element_type=F32)

        pr = proj(1) * proj(2)
        one = jnp.where(pos >= 1, pltpu.roll(pr, 1, 0), 0.0)
        two = jnp.where(pos >= 2, pltpu.roll(pr, 2, 0), 0.0)
        conv = tap[0] * two + tap[1] * one + tap[2] * pr
        gated[role, chunk(c), :] = (proj(0) * conv).astype(BF16)
        ref = gated.at[role, chunk(c)]
        start(remote(ref, ref, gone.at[6], g_r.at[c], z_dev))

    def mix_out(c):
        landed(gated.at[role, chunk(c)], g_r.at[c])
        g = jnp.concatenate([gated[0, chunk(c), :], gated[1, chunk(c), :]], axis=1)
        for s in range(n_fs):
            MP[chunk(c), s * mcols:(s + 1) * mcols] = jnp.dot(
                g, WM[s], preferred_element_type=F32
            ).astype(BF16)
        start(remote(MP.at[part(c, 1 - t)], RS.at[c], gone.at[7], sib_r.at[c], s_dev))

    def mix_pair(c):
        landed(RS.at[c], sib_r.at[c])
        BR[role, c] = (MP[part(c, t), :].astype(F32) + RS[c].astype(F32)).astype(BF16)
        start(remote(BR.at[role, c], BR.at[role, c], gone.at[8], z_r.at[c], z_dev))

    def stream_chunk(c):
        landed(BR.at[1 - role, c], z_r.at[c])
        step_rows = 32

        def body(i, _):
            rows = pl.ds(pl.multiple_of(i * step_rows, step_rows), step_rows)
            mine = pl.ds(pl.multiple_of((2 * c + t) * half + i * step_rows, step_rows), step_rows)
            branch = jnp.concatenate(
                [BR[q, c, rows, s * mcols:(s + 1) * mcols] for s in range(n_fs) for q in range(2)], axis=1
            )
            stream = tok[mine, :].astype(F32) + branch.astype(F32)
            n2[mine, :] = rms_scale(stream, ffn_gain[...]).astype(BF16)
            return 0

        lax.fori_loop(0, half // step_rows, body, 0)
        ref = n2.at[part(c, t)]
        start(remote(ref, ref, gone.at[9], n_r.at[c], s_dev))

    def ffn_rows(k, i):
        _, _, _, c0, nc, _ = pieces[k]
        cuts = 2 if nc == 2 * LANES else 1
        n = 4 * half // cuts
        for a in range(c0, c0 + nc, 2 * LANES):
            w = WG[:, :, a:a + 2 * LANES].reshape(width, 2 * LANES)
            for j in range(cuts):
                rows = pl.ds(4 * i * half + j * n, n)
                zz = jnp.dot(n2[rows, :], w, preferred_element_type=F32)
                g, u = zz[:, :LANES], zz[:, LANES:]
                hidden[rows, a // 2:a // 2 + LANES] = (g / (1.0 + jnp.exp(-g)) * u).astype(BF16)

    dn = (9, 10, 11) if role else (8, 9, 10)
    cuts = [pieces[k][3:5] for k in dn]
    groups = [
        ((f,), (0, cols)), ((x_of, y_of), cuts[0]), ((x_of, y_of), cuts[1]), ((d_of,), cuts[0]),
        ((x_of, y_of), cuts[2]), ((d_of,), cuts[1]), ((d_of,), cuts[2]),
    ]
    def span(k, hs):
        n = len(groups[k][0])
        return n, pl.ds(*groups[k][1]), pl.ds(2 * hs[0], 2 * len(hs)), pl.ds(hs[0], len(hs)), 7 * hs[0] + k

    def down_send(k, *hs):
        slots, (c0, nc) = groups[k]
        _, cs, two, _, sem = span(k, hs)
        w = jnp.concatenate([WD[s, :hid, c0:c0 + nc] for s in slots], axis=1)
        for h in hs:
            prod = jnp.dot(
                hidden[pl.ds(4 * h * half, 4 * half), :hid], w, preferred_element_type=F32
            ).astype(BF16)
            for j, s in enumerate(slots):
                for e in range(4):
                    OP[s, e % 2, 2 * h + e // 2, :, c0:c0 + nc] = prod[e * half:(e + 1) * half, j * nc:(j + 1) * nc]
        for s in slots:
            start(remote(OP.at[s, 1 - t, two, :, cs], RO.at[s, two, :, cs], gone.at[10], o_r.at[sem], s_dev))

    def down_pair(k, *hs):
        slots, _ = groups[k]
        n, cs, two, rows, sem = span(k, hs)
        landed(RO.at[pl.ds(0, n), two, :, cs], o_r.at[sem])
        for s in slots:
            for h in hs:
                c = 2 * h + 1 - p
                ZC[s, h, :, cs] = (OP[s, t, c, :, cs].astype(F32) + RO[s, c, :, cs].astype(F32)).astype(BF16)
            start(remote(ZC.at[s, rows, :, cs], RF.at[s, rows, :, cs], gone.at[11], q_r.at[sem], z_dev))

    def finish(k, *hs):
        slots, (c0, nc) = groups[k]
        n, cs, _, rows, sem = span(k, hs)
        landed(RF.at[pl.ds(0, n), rows, :, cs], q_r.at[sem])
        for s in slots:
            for h in hs:
                c = 2 * h + p
                for a in range(0, nc, LANES):
                    lo = c0 + a
                    q, at = lo // mcols, lo % mcols
                    cs = pl.ds(lo, LANES)
                    ms = pl.ds(pl.multiple_of(s * mcols + at, LANES), LANES)
                    whole = pl.ds(pl.multiple_of(s * cols + lo, LANES), LANES)
                    stream = tok[part(c, t), whole].astype(F32) + BR[q, c, :, ms].astype(F32)
                    branch = (
                        OP[s, t, c, :, cs].astype(F32)
                        + RO[s, c, :, cs].astype(F32)
                        + RF[s, h, :, cs].astype(F32)
                    )
                    out[h * half:(h + 1) * half, whole] = (stream + branch).astype(BF16)

    def later(*cs):
        for c in cs:
            landed(n2.at[part(c, 1 - t)], n_r.at[c])

    if role:
        mix_in(0)
        mix_in(1)
        mix_in(2)
        step(4, 6)
        mix_in(3)
        arrived(2, 3)
        mix_out(0)
        mix_out(1)
        mix_pair(0)
        step(5, 7)
        mix_out(2)
        mix_pair(1)
        across(4)
        mix_out(3)
        mix_pair(2)
        mix_pair(3)
        step(6, 8)
        stream_chunk(0)
        across(5)
        stream_chunk(1)
        step(7)
        later(0, 1)
        arrived(4)
        ffn_rows(4, 0)
        across(6)
        arrived(5)
        ffn_rows(5, 0)
        stream_chunk(2)
        step(8, 9, 10, 11)
        stream_chunk(3)
        across(7)
        later(2, 3)
        ffn_rows(4, 1)
        across(8)
        ffn_rows(5, 1)
        arrived(6)
        ffn_rows(6, 0)
        step(9)
        arrived(7)
        ffn_rows(7, 0)
        arrived(8)
        ffn_rows(8, 0)
        down_send(0, 0)
        step(10)
        ffn_rows(6, 1)
        down_pair(0, 0)
        ffn_rows(7, 1)
        ffn_rows(8, 1)
        down_send(0, 1)
        sides(9)
        down_pair(0, 1)
        down_send(1, 0, 1)
        down_pair(1, 0, 1)
        sides(10)
        down_send(2, 0, 1)
        step(11)
        down_pair(2, 0, 1)
        down_send(4, 0, 1)
        across(9)
        down_pair(4, 0, 1)
        across(10)
        finish(0, 0)
        finish(0, 1)
        corner(9)
        down_send(3, 0, 1)
        corner(10)
        down_send(5, 0, 1)
        down_pair(3, 0, 1)
        across(11)
        down_send(6, 0, 1)
        down_pair(5, 0, 1)
    else:
        mix_in(0)
        mix_in(1)
        step(2)
        mix_in(2)
        mix_in(3)
        step(3, 4, 5)
        arrived(2, 3)
        mix_out(0)
        mix_out(1)
        mix_pair(0)
        mix_out(2)
        mix_pair(1)
        step(4, 6)
        mix_out(3)
        mix_pair(2)
        mix_pair(3)
        stream_chunk(0)
        step(5, 7)
        stream_chunk(1)
        later(0, 1)
        arrived(4)
        ffn_rows(4, 0)
        step(6)
        stream_chunk(2)
        arrived(5)
        ffn_rows(5, 0)
        step(7, 8, 9)
        stream_chunk(3)
        later(2, 3)
        ffn_rows(4, 1)
        ffn_rows(5, 1)
        arrived(6)
        ffn_rows(6, 0)
        ffn_rows(6, 1)
        arrived(7)
        ffn_rows(7, 0)
        down_send(0, 0)
        ffn_rows(7, 1)
        down_pair(0, 0)
        down_send(0, 1)
        step(8, 10)
        down_pair(0, 1)
        step(9)
        down_send(1, 0, 1)
        down_send(2, 0, 1)
        down_pair(1, 0, 1)
        down_pair(2, 0, 1)
        finish(0, 0)
        step(10)
        down_send(4, 0, 1)
        across(8)
        across(9)
        down_send(3, 0, 1)
        down_send(5, 0, 1)
        down_pair(4, 0, 1)
        down_pair(3, 0, 1)
        down_pair(5, 0, 1)
        finish(0, 1)
        across(10)
        down_send(6, 0, 1)

    finish(1, 0, 1)
    down_pair(6, 0, 1)
    for k in (2, 4, 3, 5, 6):
        finish(k, 0, 1)
    for w, ref in enumerate((
        WA.at[pl.ds(0, 3)], WM.at[pl.ds(0, 3)], WG.at[pl.ds(0, 3), :, pl.ds(0, 2 * hid)],
        WD.at[pl.ds(0, 3), pl.ds(0, hid)], tok.at[pl.ds(0, 2 * half)], tok.at[pl.ds(0, 2 * half)],
        gated.at[role], RS, BR.at[role], n2.at[pl.ds(0, 4 * half)], RO, ZC,
    )):
        left(ref, w)


def paired_local(
    tokens, mix_gain, w_gate_b, w_gate_c, w_conv_in, conv_taps, w_mix_out, ffn_gain,
    w_ffn_gate, w_ffn_up, w_ffn_down,
):
    chip_rows, width = tokens.shape
    n_fs = lax.axis_size("fs")
    rows_d = w_gate_b.shape[0]
    ch = w_gate_b.shape[1] // 2
    units = inner_units(w_ffn_gate.shape[1])
    hid = units * LANES
    cols = w_mix_out.shape[1]
    half = chip_rows // 4
    group = 2 * chip_rows

    def vmem(*shape):
        return pltpu.VMEM(shape, BF16)

    def dma(*shape):
        return pltpu.SemaphoreType.DMA(shape)

    return pl.pallas_call(
        layer_kernel,
        out_shape=pltpu.VMEM((2 * half, width), BF16),
        in_specs=[pl.BlockSpec(memory_space=pl.ANY)] * 11,
        out_specs=pl.BlockSpec(memory_space=pltpu.VMEM),
        scratch_shapes=[
            vmem(group, width),
            vmem(group, width),
            vmem(group, width),
            vmem(n_fs, rows_d, 3 * ch),
            vmem(n_fs, 2 * ch, cols // 2),
            vmem(n_fs, rows_d, 2 * hid),
            vmem(n_fs, hid, cols),
            vmem(2, group, ch),
            vmem(group, width // 2),
            vmem(N_CHUNKS, half, width // 2),
            vmem(2, N_CHUNKS, half, width // 2),
            vmem(group, hid),
            vmem(n_fs, 2, N_CHUNKS, half, cols),
            vmem(n_fs, N_CHUNKS, half, cols),
            vmem(n_fs, 2, half, cols),
            vmem(n_fs, 2, half, cols),
            pltpu.VMEM((1, width), F32),
            pltpu.VMEM(conv_taps.shape, F32),
            pltpu.VMEM((1, width), F32),
            dma(10),
            dma(12),
            *[dma(N_PIECES)] * 4,
            *[dma(2)] * 2,
            *[dma(N_CHUNKS)] * 4,
            *[dma(8)] * 2,
        ],
        compiler_params=pltpu.CompilerParams(
            collective_id=0, has_side_effects=True, vmem_limit_bytes=60 * 2**20
        ),
    )(
        tokens, w_gate_b, w_gate_c, w_conv_in, w_mix_out, w_ffn_gate, w_ffn_up, w_ffn_down,
        mix_gain.reshape(1, width), conv_taps, ffn_gain.reshape(1, width),
    )


def causal_mix(product_in, conv_taps):
    shaped = product_in.reshape(product_in.shape[0] // LEN, LEN, product_in.shape[1])
    padded = jnp.pad(shaped, ((0, 0), (2, 0), (0, 0)))
    convolved = (
        conv_taps[0] * padded[:, :-2]
        + conv_taps[1] * padded[:, 1:-1]
        + conv_taps[2] * padded[:, 2:]
    )
    return convolved.reshape(product_in.shape)


def general_local(
    tokens, mix_gain, w_gate_b, w_gate_c, w_conv_in, conv_taps, w_mix_out, ffn_gain,
    w_ffn_gate, w_ffn_up, w_ffn_down,
):
    def scatter(product):
        return lax.psum_scatter(
            product.astype(BF16), "tp", scatter_dimension=0, tiled=True
        ).astype(F32)

    def dot(a, b):
        return jnp.dot(a, b, preferred_element_type=F32)

    def rows(w):
        return lax.all_gather(w, "fs", axis=0, tiled=True)

    normed = rms_scale(tokens.astype(F32), mix_gain).astype(BF16)
    gate_b, gate_c, conv_in = (dot(normed, rows(w)) for w in (w_gate_b, w_gate_c, w_conv_in))
    gated = (gate_b * causal_mix(gate_c * conv_in, conv_taps)).astype(BF16)
    row_count = normed.shape[0] // lax.axis_size("tp")
    branch = scatter(dot(gated, lax.all_gather(w_mix_out, "fs", axis=1, tiled=True)))
    own = lax.dynamic_slice_in_dim(tokens, lax.axis_index("tp") * row_count, row_count, 0)
    stream = own.astype(F32) + branch
    normed_two = lax.all_gather(
        rms_scale(stream, ffn_gain).astype(BF16), "tp", axis=0, tiled=True
    )
    hidden = (jax.nn.silu(dot(normed_two, rows(w_ffn_gate))) * dot(normed_two, rows(w_ffn_up))).astype(BF16)
    ffn_branch = scatter(dot(hidden, lax.all_gather(w_ffn_down, "fs", axis=1, tiled=True)))
    return (stream + ffn_branch).astype(BF16)


def solution(mesh):
    in_specs = (
        P(("rep", "fs"), None),
        P(),
        P("fs", "tp"),
        P("fs", "tp"),
        P("fs", "tp"),
        P(None, "tp"),
        P("tp", "fs"),
        P(),
        P("fs", "tp"),
        P("fs", "tp"),
        P("tp", "fs"),
    )
    out_specs = P(("rep", "fs", "tp"), None)
    size = mesh.shape
    square = size["tp"] == 2 and size["fs"] == 4 and size["rep"] == 4

    def local(*arrays):
        rows, width = arrays[0].shape
        channels, hidden = arrays[2].shape[1], arrays[8].shape[1]
        fits = (
            square
            and rows % (4 * LEN) == 0
            and channels % (2 * LANES) == 0
            and hidden % LANES == 0
            and hidden >= 11 * LANES
            and width % (16 * LANES) == 0
        )
        return (paired_local if fits else general_local)(*arrays)

    return jax.shard_map(local, mesh=mesh, in_specs=in_specs, out_specs=out_specs, check_vma=False)
```
